32 devices in a mesh: fs: 8 (over z, x), tp: 4 (over y, core).
Axes of the slice: x: 2, y: 2, z: 4, core: 2. Of those that a mesh axis runs over, the one named last changes fastest.
Arguments:
- tokens: bfloat16 [320, 4096], P('fs'), may hold values from -6 to 6
- routes: int32 [320, 2], P('fs'), may hold values from 0 to 3, all different within a row; in each aligned block of 40 rows (0 to 39, 40 to 79, ...) at most 30 rows name the same one
- route_logits: float32 [320, 2], P('fs'), may hold values from -6 to 6
- norm_gain: float32 [4096], P('fs'), may hold values from 0.1 to 1.9
- gate_weight: float32 [4, 4096, 8192], P(None, 'fs', 'tp'), may hold values from -0.09375 to 0.09375
- up_weight: float32 [4, 4096, 8192], P(None, 'fs', 'tp'), may hold values from -0.09375 to 0.09375
- down_weight: float32 [4, 4096, 8192], P(None, 'fs', 'tp'), may hold values from -0.0625 to 0.0625
Outputs:
- mixed: bfloat16 [320, 4096], P('fs', 'tp')
- gate_sampler: bfloat16 [4, 4096, 8192], P('tp', None, 'fs')
- up_sampler: bfloat16 [4, 4096, 8192], P('tp', None, 'fs')
- down_sampler: bfloat16 [4, 4096, 8192], P('tp', None, 'fs')
The draws below stay inside these ranges and needn't reach their ends.
Inputs may be any that keep to these rules, and one draw needn't show every extreme that they name: `routes`: the 2 experts of a token differ. Within the tokens of one index of fs (aligned blocks of 40 rows) no expert is named by more than 30 tokens.
All inputs are finite; a program needn't handle non-finite values.
Results may differ from the reference program's by a relative error of at most 0.01.
Values may be sent and summed in bfloat16 or wider, within the bound.
A program may use at most 192 MiB of HBM per device.

```python
import math
import jax
import jax.numpy as jnp
import numpy as np
from jax import lax

D = 4096
FF = 8192
EXPERTS = 4
TOPK = 2
TOK_DEV = 40
CAP = 30
TOKENS = 320
N_TP = 4


def block_scale(own_key, extent, pieces, least, high):
    gain = 1.0
    for dim, parts in pieces:
        heights = jax.random.uniform(jax.random.fold_in(jax.random.fold_in(own_key, 6), dim), (parts,), jnp.float32, least / len(pieces), high / len(pieces))
        gain = gain * jnp.repeat(jnp.exp(heights), extent[dim] // parts).reshape((-1,) + (1,) * (len(extent) - 1 - dim))
    return gain


def assign_block(own_key, own, number, rows, number_of, top, limit, lean):
    order = jax.random.permutation(own_key, number_of)
    heavy_load, usual = portions_of(number_of, rows * top, limit, lean, True), portions_of(number_of, rows * top, limit, lean, False)
    places = jnp.arange(number_of)

    def named(sizes, offset_by):
        used = int((sizes > 0).sum())
        fixed = max(1, used // 4)
        moved = fixed + (places - fixed + offset_by * (used - fixed)) % max(1, number_of - fixed)
        return jnp.zeros((number_of,), jnp.int32).at[order[jnp.where(places < fixed, places, moved)]].set(jnp.asarray(sizes, jnp.int32))

    sizes = jnp.where(number % 4 == 0, named(heavy_load, number // 4), named(usual, number - number // 4 - 1))
    mixed = jax.random.permutation(jax.random.fold_in(own, 3), number_of)
    donor, sink = mixed[0:number_of // 2 * 2:2], mixed[1:number_of // 2 * 2:2]
    room = jnp.minimum(sizes[donor] - 1, limit - sizes[sink]) // 2
    room = jnp.where((donor == order[0]) | (sink == order[0]) | (sizes[sink] == 0), 0, jnp.maximum(room, 0))
    moved = jax.random.randint(jax.random.fold_in(own, 4), (number_of // 2,), 0, 1 << 20) % (room + 1)
    sizes = sizes.at[donor].add(-moved).at[sink].add(moved)
    labels = jnp.searchsorted(jnp.cumsum(sizes), jnp.arange(rows * top), side="right").astype(jnp.int32)
    grid = labels.reshape(top, rows).T
    grid = grid[jax.random.permutation(jax.random.fold_in(own, 1), rows)]
    offset_by = jax.random.randint(jax.random.fold_in(own, 2), (rows, 1), 0, top)
    return jnp.take_along_axis(grid, (jnp.arange(top)[None, :] + offset_by) % top, axis=1)


def portions_of(count, total, most, slope, full):
    loads = [(1 << 20) // math.isqrt(rank ** slope) + 1 for rank in range(1, count + 1)]
    largest = most if full else min(most, max(-(-total // count), total * loads[0] // sum(loads)))
    least = 1 if total - largest >= count - 1 else 0
    holding, spare = [largest] + [least] * (count - 1), total - largest - least * (count - 1)
    while spare > 0:
        free = [i for i in range(1, count) if holding[i] < largest] or [i for i in range(1, count) if holding[i] < most]
        mass, remaining = sum([loads[i] for i in free]), spare
        for i in free:
            extra = min(most - holding[i], max(1, remaining * loads[i] // mass), spare)
            holding[i] = holding[i] + extra
            spare = spare - extra
    return np.array(holding)


def centred(key, extent, scale, reach, cuts=(), held_as=jnp.bfloat16):
    drawn = jax.random.normal(key, extent, jnp.float32) * scale
    if len(cuts) > 0:
        drawn = block_scale(key, extent, cuts, -0.22, 0.18) * drawn
    return jnp.clip(drawn, min=-reach, max=reach).astype(held_as)


def setup_inputs(seed: int = 0) -> dict:
    arg_keys = jax.random.split(jax.random.key(seed), 8)
    tokens = centred(arg_keys[0], (TOKENS, D), 1.0, 6.0, ((0, 8),))
    routes_keys = jax.random.split(jax.random.fold_in(arg_keys[1], 1), TOKENS // TOK_DEV)
    routes_turns = jax.random.permutation(jax.random.fold_in(arg_keys[1], 3), TOKENS // TOK_DEV)
    routes = jax.vmap(lambda own, number: assign_block(jax.random.fold_in(arg_keys[1], 2), own, number, TOK_DEV, EXPERTS, TOPK, CAP, 2))(routes_keys, routes_turns).reshape((TOKENS, TOPK))
    route_logits = centred(arg_keys[2], (TOKENS, TOPK), 1.5, 6.0, ((0, 8),), jnp.float32)
    norm_gain = jnp.clip(1.0 + 0.18 * jax.random.normal(arg_keys[3], (D,), jnp.float32), 0.1, 1.9)
    gate_weight = centred(arg_keys[4], (EXPERTS, D, FF), D ** -0.5, 0.09375, ((1, 8), (2, 4)), jnp.float32)
    up_weight = centred(arg_keys[5], (EXPERTS, D, FF), D ** -0.5, 0.09375, ((1, 8), (2, 4)), jnp.float32)
    down_weight = centred(arg_keys[6], (EXPERTS, D, FF), FF ** -0.5, 0.0625, ((1, 8), (2, 4)), jnp.float32)
    return {"tokens": tokens, "routes": routes, "route_logits": route_logits, "norm_gain": norm_gain, "gate_weight": gate_weight, "up_weight": up_weight, "down_weight": down_weight}


def arrange(matrix):
    experts, width, hidden_units = matrix.shape
    block = hidden_units // N_TP
    split = matrix.reshape(experts, width, N_TP, block)
    return jnp.transpose(split, (2, 1, 0, 3)).reshape(N_TP, width, experts * block)

def reference(tokens, routes, route_logits, norm_gain, gate_weight, up_weight, down_weight):
    gain_cols = norm_gain.astype(jnp.float32)[None, :, None]
    folded_gate = (gate_weight * gain_cols).astype(jnp.bfloat16)
    folded_up = (up_weight * gain_cols).astype(jnp.bfloat16)
    rounded_down = down_weight.astype(jnp.bfloat16)
    tok_float = tokens.astype(jnp.float32)
    normed = (tok_float * lax.rsqrt(lax.optimization_barrier(jnp.mean(tok_float * tok_float, axis=1, keepdims=True)) + 1e-05)).astype(jnp.bfloat16)
    shares = jax.nn.sigmoid(route_logits - route_logits[:, ::-1])
    mixed = jnp.zeros((tokens.shape[0], tokens.shape[1]), jnp.float32)
    for expert in range(EXPERTS):
        gate_act = jnp.dot(normed, folded_gate[expert], preferred_element_type=jnp.float32)
        up_act = jnp.dot(normed, folded_up[expert], preferred_element_type=jnp.float32)
        hidden = (jax.nn.silu(gate_act) * up_act).astype(jnp.bfloat16)
        expert_out = lax.dot_general(hidden, rounded_down[expert], (((1,), (1,)), ((), ())), preferred_element_type=jnp.float32)
        weight = lax.optimization_barrier(jnp.sum(jnp.where(routes == expert, shares, 0.0), axis=1))
        mixed = mixed + weight[:, None] * expert_out
    return (mixed.astype(jnp.bfloat16), arrange(folded_gate), arrange(folded_up), arrange(rounded_down))
```

```python
import functools

import jax
import jax.numpy as jnp
from jax import lax
from jax.experimental import pallas as pl
from jax.experimental.pallas import tpu as pltpu
from jax.sharding import PartitionSpec as P

MESH = pl.DeviceIdType.MESH
F32, BF16 = jnp.float32, jnp.bfloat16


def wait_bytes(ref, sem):
    pltpu.make_async_copy(ref, ref, sem).wait()


def loop(count, body):
    def step(i, carry):
        body(i)
        return carry

    lax.fori_loop(0, count, step, 0)


def fused_kernel(
    fs_count, tp_count, experts, pieces,
    tok_ref, routes_ref, logits_ref, gain_ref, gate_hbm, up_hbm, down_hbm,
    mixed_out, gate_out, up_out, down_out,
    stage, gate_send, up_send, down_send, down_recv, wbuf,
    xown, xcol, x_all, act, hidden, part, rs_recv, total, home,
    load_sem, send_sem, recv_sem, keep_sem, down_sem, down_keep, x_sem, wload_sem,
    rs_send_sem, rs_recv_sem, home_send, home_recv,
):
    me, my_tp = lax.axis_index("fs"), lax.axis_index("tp")
    spread = fs_count // experts
    mine, inner = me // spread, lax.rem(me, spread)
    group = spread * tp_count
    index = inner * tp_count + my_tp
    half = fs_count // 2
    side = me // half
    share = fs_count // tp_count
    own, model = tok_ref.shape
    width, block = stage.shape[1], stage.shape[2]
    rows = width // pieces
    tokens = fs_count * own
    pairs = tp_count // 2
    rounds = 2 * pieces
    owner_fs, owner_tp = me // tp_count, lax.rem(me, tp_count)

    def send_order(step):
        far = (1 - side) * half + lax.rem(me + step, half)
        near = side * half + lax.rem(me + 1 + step, half)
        return jnp.where(step < half, far, near)

    def near_source(k):
        return side * half + lax.rem(me + 2 * half - 1 - k, half)

    def far_source(k):
        return (1 - side) * half + lax.rem(me + half - k, half)

    def gather_peer(s):
        other = lax.rem(my_tp * share + lax.rem(inner, share) + s, fs_count)
        fs = mine * spread + (inner // share) * share + lax.rem(other, share)
        return fs, other // share

    def plane_peer(i):
        return mine * spread + i // tp_count, lax.rem(i, tp_count)

    barrier = pltpu.get_barrier_semaphore()

    def signal(fs, tp):
        pl.semaphore_signal(
            barrier, inc=1, device_id={"fs": fs, "tp": tp}, device_id_type=MESH
        )

    def load(hbm, step, slot):
        dst = send_order(step)
        column = pl.multiple_of(lax.rem(dst, spread) * block, block)
        return pltpu.make_async_copy(
            hbm.at[dst // spread, :, pl.ds(column, block)], stage.at[slot], load_sem.at[slot]
        )

    load(gate_hbm, 0, 0).start()
    loop(fs_count - 1, lambda s: signal(lax.rem(me + 1 + s, fs_count), my_tp))

    def greet(s):
        fs, tp = plane_peer(lax.rem(index + 1 + s, group))
        signal(fs, tp)

    loop(group - 1, greet)

    def sender_of(e):
        return e * spread + owner_fs, owner_tp

    def is_self(fs, tp):
        return jnp.logical_and(fs == me, tp == my_tp)

    for e in range(experts):
        fs, tp = sender_of(e)

        @pl.when(jnp.logical_not(is_self(fs, tp)))
        def _(fs=fs, tp=tp):
            signal(fs, tp)

    tok = tok_ref[...].astype(F32)
    scale = lax.rsqrt(jnp.mean(tok * tok, axis=1, keepdims=True) + 1e-05)
    for j in range(share):
        column = pl.multiple_of((my_tp * share + j) * width, width)
        cols = tok_ref[:, pl.ds(column, width)].astype(F32)
        xown[j] = (cols * scale).astype(BF16)
    xcol[me] = xown[lax.rem(inner, share)]

    homes = jnp.where(index < fs_count, tp_count, 0) - jnp.where(index == me, 1, 0)
    pl.semaphore_wait(barrier, fs_count + group - 2 + homes)

    def x_send(s):
        dst = send_order(s)
        pltpu.make_async_remote_copy(
            src_ref=xown.at[lax.rem(lax.rem(dst, spread), share)], dst_ref=xcol.at[me],
            send_sem=x_sem.at[0], recv_sem=x_sem.at[1], device_id={"fs": dst},
            device_id_type=MESH,
        ).start()

    loop(fs_count - 1, x_send)

    def block_copy(m, held, out, dst):
        return pltpu.make_async_remote_copy(
            src_ref=held.at[dst], dst_ref=out.at[me], send_sem=send_sem.at[m],
            recv_sem=recv_sem.at[m, me], device_id={"fs": dst}, device_id_type=MESH,
        )

    def piece_copy(p, dst):
        span = pl.ds(pl.multiple_of(p * rows, rows), rows)
        return pltpu.make_async_remote_copy(
            src_ref=down_send.at[dst, span], dst_ref=down_recv.at[me, span],
            send_sem=send_sem.at[2], recv_sem=down_sem.at[p, me], device_id={"fs": dst},
            device_id_type=MESH,
        )

    def convert(m, hbm, following):
        def body(step):
            slot = lax.rem(m * fs_count + step, 2)
            dst = send_order(step)

            @pl.when(step + 1 < fs_count)
            def _():
                load(hbm, step + 1, 1 - slot).start()

            if following is not None:

                @pl.when(step + 1 == fs_count)
                def _():
                    load(following, 0, 1 - slot).start()

            load(hbm, step, slot).wait()
            if m < 2:
                held, out = ((gate_send, gate_out), (up_send, up_out))[m]
                held[dst] = (stage[slot] * gain_ref[...]).astype(BF16)

                @pl.when(dst == me)
                def _():
                    pltpu.make_async_copy(held.at[me], out.at[me], keep_sem.at[m]).start()

                @pl.when(dst != me)
                def _():
                    block_copy(m, held, out, dst).start()
            else:

                @pl.when(dst == me)
                def _():
                    down_recv[me] = stage[slot].astype(BF16)

                @pl.when(dst != me)
                def _():
                    down_send[dst] = stage[slot].astype(BF16)

        loop(fs_count, body)

    convert(0, gate_hbm, up_hbm)

    wait_bytes(xcol.at[pl.ds(0, fs_count - 1)], x_sem.at[1])
    held_part = my_tp * share + lax.rem(inner, share)

    def x_gather(s):
        fs, tp = gather_peer(s + 1)
        pltpu.make_async_remote_copy(
            src_ref=xcol, dst_ref=x_all.at[held_part], send_sem=x_sem.at[2],
            recv_sem=x_sem.at[3], device_id={"fs": fs, "tp": tp}, device_id_type=MESH,
        ).start()

    loop(fs_count - 1, x_gather)
    x_all[held_part] = xcol[...]

    convert(1, up_hbm, down_hbm)
    convert(2, down_hbm, None)
    loop(pieces, lambda p: loop(fs_count - 1, lambda s: piece_copy(p, send_order(s)).start()))

    wait_bytes(x_all.at[pl.ds(0, fs_count - 1)], x_sem.at[3])

    def project(m, held, out, a):
        act[a] = jnp.zeros_like(act[a])

        def body(k):
            g = jnp.where(k < half, near_source(k), far_source(k - half))

            @pl.when(g == me)
            def _():
                wait_bytes(held.at[me], keep_sem.at[m])

            @pl.when(g != me)
            def _():
                wait_bytes(out.at[g], recv_sem.at[m, g])

            fetch = pltpu.make_async_copy(out.at[g], wbuf, wload_sem)
            fetch.start()
            x = x_all[g].astype(F32).reshape(tokens, width).astype(BF16)
            fetch.wait()
            act[a] += jnp.dot(x, wbuf[...], preferred_element_type=F32)

        loop(fs_count, body)

    project(0, gate_send, gate_out, 0)
    project(1, up_send, up_out, 1)
    gate = act[0]
    hidden[...] = (gate / (1.0 + jnp.exp(-gate)) * act[1]).astype(BF16)

    def base_of(r):
        return jnp.where(lax.rem(r, 2) == 0, side, 1 - side) * half

    def finish(r):
        p = r // 2
        wait_bytes(rs_recv.at[r], rs_recv_sem.at[r])

        def add(s, acc):
            return acc + rs_recv[r, s].astype(F32)

        acc = lax.fori_loop(0, group - 1, add, part[r, index].astype(F32))
        total[r] = acc.astype(BF16)
        for q in range(pairs):
            tp = base_of(r) // share + q

            @pl.when(is_self(index, tp))
            def _(q=q):
                home[mine, p] = total[r, pl.ds(q * share, share)]

            @pl.when(jnp.logical_not(is_self(index, tp)))
            def _(q=q, tp=tp):
                home_copy(r, q, tp).start()

    def home_copy(r, q, tp):
        return pltpu.make_async_remote_copy(
            src_ref=total.at[r, pl.ds(q * share, share)], dst_ref=home.at[mine, r // 2],
            send_sem=home_send.at[r, q], recv_sem=home_recv.at[r // 2, mine],
            device_id={"fs": index, "tp": tp}, device_id_type=MESH,
        )

    def run_round(r):
        p = r // 2
        span = pl.ds(pl.multiple_of(p * rows, rows), rows)

        def item(k):
            g = jnp.where(lax.rem(r, 2) == 0, near_source(k), far_source(k))

            @pl.when(g != me)
            def _():
                wait_bytes(down_recv.at[g, span], down_sem.at[p, g])

            pltpu.make_async_copy(
                down_recv.at[g, span], down_out.at[g, span], down_keep
            ).start()
            out = lax.dot_general(
                hidden[...], down_recv[g, span], (((1,), (1,)), ((), ())),
                preferred_element_type=F32,
            )
            part[r, :, g - base_of(r)] = out.reshape(fs_count, own, rows).astype(BF16)

        loop(half, item)

        def rs_send(s):
            i = lax.rem(index + 1 + s, fs_count)

            @pl.when(i != index)
            def _():
                fs, tp = plane_peer(i)
                slot = lax.rem(index + 2 * group - i - 1, group)
                pltpu.make_async_remote_copy(
                    src_ref=part.at[r, i], dst_ref=rs_recv.at[r, slot],
                    send_sem=rs_send_sem.at[r], recv_sem=rs_recv_sem.at[r],
                    device_id={"fs": fs, "tp": tp}, device_id_type=MESH,
                ).start()

        loop(fs_count, rs_send)

        @pl.when(jnp.logical_and(r > 0, index < fs_count))
        def _():
            finish(r - 1)

    loop(rounds, run_round)

    @pl.when(index < fs_count)
    def _():
        finish(rounds - 1)

    first, second = logits_ref[:, 0:1], logits_ref[:, 1:2]
    share_first = 1.0 / (1.0 + jnp.exp(second - first))
    share_second = 1.0 / (1.0 + jnp.exp(first - second))
    for p in range(pieces):
        mixed = [jnp.zeros((own, rows), F32)] * share
        for e in range(experts):

            @pl.when(jnp.logical_not(is_self(*sender_of(e))))
            def _(e=e, p=p):
                wait_bytes(home.at[e, p], home_recv.at[p, e])

            weight = jnp.where(routes_ref[:, 0:1] == e, share_first, 0.0) + jnp.where(
                routes_ref[:, 1:2] == e, share_second, 0.0
            )
            for j in range(share):
                mixed[j] = mixed[j] + weight * home[e, p, j].astype(F32)
        for j in range(share):
            column = j * width + p * rows
            mixed_out[:, column : column + rows] = mixed[j].astype(BF16)

    wait_bytes(down_recv, down_keep)
    wait_bytes(xcol.at[pl.ds(0, fs_count - 1)], x_sem.at[0])
    wait_bytes(x_all.at[pl.ds(0, fs_count - 1)], x_sem.at[2])
    for m, held in enumerate((gate_send, up_send, down_send)):
        wait_bytes(held.at[pl.ds(0, fs_count - 1)], send_sem.at[m])

    def drain(r):
        @pl.when(index < fs_count)
        def _():
            wait_bytes(part.at[r, pl.ds(0, fs_count - 1)], rs_send_sem.at[r])
            for q in range(pairs):
                tp = base_of(r) // share + q

                @pl.when(jnp.logical_not(is_self(index, tp)))
                def _(q=q):
                    wait_bytes(total.at[r, pl.ds(q * share, share)], home_send.at[r, q])

        @pl.when(index >= fs_count)
        def _():
            wait_bytes(part.at[r], rs_send_sem.at[r])

    loop(rounds, drain)


def per_device(tokens, routes, route_logits, norm_gain, gate_weight, up_weight, down_weight):
    experts, width, columns = gate_weight.shape
    fs_count, tp_count = lax.axis_size("fs"), lax.axis_size("tp")
    spread = fs_count // experts
    block = columns // spread
    own, model = tokens.shape
    group = spread * tp_count
    half, share = fs_count // 2, fs_count // tp_count
    pieces = max(1, width // 128)
    rows = width // pieces
    rounds = 2 * pieces
    dma = pltpu.SemaphoreType.DMA
    vmem = pl.BlockSpec(memory_space=pltpu.VMEM)
    anywhere = pl.BlockSpec(memory_space=pl.ANY)
    landed = jax.ShapeDtypeStruct((fs_count, width, block), BF16)
    mixed, *landings = pl.pallas_call(
        functools.partial(fused_kernel, fs_count, tp_count, experts, pieces),
        in_specs=[vmem] * 4 + [anywhere] * 3,
        out_specs=[vmem] + [anywhere] * 3,
        out_shape=[jax.ShapeDtypeStruct((own, model // tp_count), BF16)] + [landed] * 3,
        scratch_shapes=[
            pltpu.VMEM((2, width, block), F32),
            pltpu.VMEM((fs_count, width, block), BF16),
            pltpu.VMEM((fs_count, width, block), BF16),
            pltpu.VMEM((fs_count, width, block), BF16),
            pltpu.VMEM((fs_count, width, block), BF16),
            pltpu.VMEM((width, block), BF16),
            pltpu.VMEM((share, own, width), BF16),
            pltpu.VMEM((fs_count, own, width), BF16),
            pltpu.VMEM((fs_count, fs_count, own, width), BF16),
            pltpu.VMEM((2, fs_count * own, block), F32),
            pltpu.VMEM((fs_count * own, block), BF16),
            pltpu.VMEM((rounds, fs_count, half, own, rows), BF16),
            pltpu.VMEM((rounds, group - 1, half, own, rows), BF16),
            pltpu.VMEM((rounds, half, own, rows), BF16),
            pltpu.VMEM((experts, pieces, share, own, rows), BF16),
            dma((2,)), dma((3,)), dma((2, fs_count)), dma((2,)), dma((pieces, fs_count)), dma,
            dma((4,)), dma, dma((rounds,)), dma((rounds,)), dma((rounds, tp_count // 2)),
            dma((pieces, experts)),
        ],
        compiler_params=pltpu.CompilerParams(
            collective_id=0, has_side_effects=True, vmem_limit_bytes=63 * 1024 * 1024
        ),
    )(
        tokens, routes, route_logits, norm_gain[:, None], gate_weight, up_weight, down_weight
    )
    return (mixed, *(x.reshape(1, fs_count * width, block) for x in landings))


def solution(mesh):
    in_specs = (
        P("fs", None),
        P("fs", None),
        P("fs", None),
        P("fs"),
        P(None, "fs", "tp"),
        P(None, "fs", "tp"),
        P(None, "fs", "tp"),
    )
    out_specs = (P("fs", "tp"), P("tp", None, "fs"), P("tp", None, "fs"), P("tp", None, "fs"))
    return jax.shard_map(
        per_device, mesh=mesh, in_specs=in_specs, out_specs=out_specs, check_vma=False
    )
```

```python
import functools

import jax
import jax.numpy as jnp
from jax import lax
from jax.experimental import pallas as pl
from jax.experimental.pallas import tpu as pltpu
from jax.sharding import PartitionSpec as P

MESH = pl.DeviceIdType.MESH
F32, BF16 = jnp.float32, jnp.bfloat16
VMEM_BYTES = 60 * 1024 * 1024


def wait_bytes(ref, sem):
    pltpu.make_async_copy(ref, ref, sem).wait()


def loop(count, body):
    def step(i, carry):
        body(i)
        return carry

    lax.fori_loop(0, count, step, 0)


def store_kernel(*refs):
    count = (len(refs) - 1) // 2
    held, out, sem = refs[:count], refs[count : 2 * count], refs[-1]
    pltpu.make_async_copy(held[0], out[0], sem.at[0]).start()
    for i in range(1, count):
        for g in range(held[i].shape[0]):
            pltpu.make_async_copy(held[i].at[g], out[i].at[g], sem.at[i]).start()
    for i in range(count):
        pltpu.make_async_copy(held[i], out[i], sem.at[i]).wait()


def fused_kernel(
    fs_count, tp_count, experts, pieces,
    tok_ref, routes_ref, logits_ref, gain_ref, gate_hbm, up_hbm, down_hbm,
    mixed_out, gate_out, up_out, down_out, up_send, down_send,
    stage, gate_send, packed, turn, gain_col,
    xown, xcol, x_all, act, hidden, part, rs_recv, total, home,
    load_sem, store_sem, send_sem, recv_sem, down_sem, x_sem,
    rs_send_sem, rs_recv_sem, home_send, home_recv,
):
    me, my_tp = lax.axis_index("fs"), lax.axis_index("tp")
    spread = fs_count // experts
    mine, inner = me // spread, lax.rem(me, spread)
    group = spread * tp_count
    index = inner * tp_count + my_tp
    half = fs_count // 2
    side = me // half
    share = fs_count // tp_count
    own, model = tok_ref.shape
    width, block = stage.shape[1], stage.shape[2]
    rows = width // pieces
    tokens = fs_count * own
    pairs = tp_count // 2
    rounds = 2 * pieces
    owner_fs, owner_tp = me // tp_count, lax.rem(me, tp_count)

    def send_order(step):
        return lax.rem(me + half + step, fs_count)

    def near_source(k):
        return side * half + lax.rem(me + 2 * half - 1 - k, half)

    def far_source(k):
        return (1 - side) * half + lax.rem(me + half - k, half)

    def gather_peer(s):
        other = lax.rem(my_tp * share + lax.rem(inner, share) + s, fs_count)
        fs = mine * spread + (inner // share) * share + lax.rem(other, share)
        return fs, other // share

    def plane_peer(i):
        return mine * spread + i // tp_count, lax.rem(i, tp_count)

    barrier = pltpu.get_barrier_semaphore()

    def signal(fs, tp):
        pl.semaphore_signal(
            barrier, inc=1, device_id={"fs": fs, "tp": tp}, device_id_type=MESH
        )

    def load(hbm, step, slot):
        dst = send_order(step)
        column = pl.multiple_of(lax.rem(dst, spread) * block, block)
        return pltpu.make_async_copy(
            hbm.at[dst // spread, :, pl.ds(column, block)], stage.at[slot], load_sem.at[slot]
        )

    load(gate_hbm, 0, 0).start()
    loop(fs_count - 1, lambda s: signal(lax.rem(me + 1 + s, fs_count), my_tp))

    def greet(s):
        fs, tp = plane_peer(lax.rem(index + 1 + s, group))
        signal(fs, tp)

    loop(group - 1, greet)

    def sender_of(e):
        return e * spread + owner_fs, owner_tp

    def is_self(fs, tp):
        return jnp.logical_and(fs == me, tp == my_tp)

    for e in range(experts):
        fs, tp = sender_of(e)

        @pl.when(jnp.logical_not(is_self(fs, tp)))
        def _(fs=fs, tp=tp):
            signal(fs, tp)

    turn[...] = jnp.zeros_like(turn)
    turn[: gain_ref.shape[0]] = gain_ref[...]
    turned = turn[...].T
    for q in range(width // 128):
        gain_col[q * 128 : (q + 1) * 128] = turned[:, q : q + 1]

    tok = tok_ref[...].astype(F32)
    scale = lax.rsqrt(jnp.mean(tok * tok, axis=1, keepdims=True) + 1e-05)
    for j in range(share):
        column = pl.multiple_of((my_tp * share + j) * width, width)
        cols = tok_ref[:, pl.ds(column, width)].astype(F32)
        xown[j] = (cols * scale).astype(BF16)
    xcol[me] = xown[lax.rem(inner, share)]

    homes = jnp.where(index < fs_count, tp_count, 0) - jnp.where(index == me, 1, 0)
    pl.semaphore_wait(barrier, fs_count + group - 2 + homes)

    def x_send(s):
        dst = lax.rem(me + 1 + s, fs_count)
        pltpu.make_async_remote_copy(
            src_ref=xown.at[lax.rem(lax.rem(dst, spread), share)], dst_ref=xcol.at[me],
            send_sem=x_sem.at[0], recv_sem=x_sem.at[1], device_id={"fs": dst},
            device_id_type=MESH,
        ).start()

    loop(fs_count - 1, x_send)

    def block_copy(m, held, out, dst):
        return pltpu.make_async_remote_copy(
            src_ref=held.at[dst], dst_ref=out.at[me], send_sem=send_sem.at[m],
            recv_sem=recv_sem.at[m, me], device_id={"fs": dst}, device_id_type=MESH,
        )

    def piece_copy(p, dst):
        span = pl.ds(pl.multiple_of(p * rows, rows), rows)
        return pltpu.make_async_remote_copy(
            src_ref=down_send.at[dst, span], dst_ref=down_out.at[me, span],
            send_sem=send_sem.at[2], recv_sem=down_sem.at[p, me], device_id={"fs": dst},
            device_id_type=MESH,
        )

    def convert(m, hbm, following):
        def body(step):
            slot = lax.rem(m * fs_count + step, 2)
            dst = send_order(step)

            @pl.when(step + 1 < fs_count)
            def _():
                load(hbm, step + 1, 1 - slot).start()

            if following is not None:

                @pl.when(step + 1 == fs_count)
                def _():
                    load(following, 0, 1 - slot).start()

            load(hbm, step, slot).wait()
            held, out = ((gate_send, gate_out), (up_send, up_out), (down_send, down_out))[m]
            block_f32 = stage[slot]
            if m < 2:
                block_f32 = block_f32 * gain_col[...]
            rounded = block_f32.astype(BF16)

            @pl.when(dst == me)
            def _():
                out[me] = rounded

            @pl.when(dst != me)
            def _():
                if m == 0:
                    held[dst] = rounded
                    block_copy(m, held, out, dst).start()
                else:
                    packed[slot] = rounded
                    store(held, step).start()

            if m > 0:

                @pl.when(jnp.logical_and(step > 0, send_order(step - 1) != me))
                def _():
                    stored(m, held, out, step - 1)

        def store(held, step):
            slot = lax.rem(m * fs_count + step, 2)
            return pltpu.make_async_copy(
                packed.at[slot], held.at[send_order(step)], store_sem.at[slot]
            )

        def stored(m, held, out, step):
            store(held, step).wait()
            if m == 1:
                block_copy(m, held, out, send_order(step)).start()

        loop(fs_count, body)
        if m > 0:
            held, out = ((up_send, up_out), (down_send, down_out))[m - 1]

            @pl.when(send_order(fs_count - 1) != me)
            def _():
                stored(m, held, out, fs_count - 1)

    convert(0, gate_hbm, up_hbm)

    wait_bytes(xcol.at[pl.ds(0, fs_count - 1)], x_sem.at[1])
    held_part = my_tp * share + lax.rem(inner, share)

    def x_gather(s):
        fs, tp = gather_peer(s + 1)
        pltpu.make_async_remote_copy(
            src_ref=xcol, dst_ref=x_all.at[held_part], send_sem=x_sem.at[2],
            recv_sem=x_sem.at[3], device_id={"fs": fs, "tp": tp}, device_id_type=MESH,
        ).start()

    loop(fs_count - 1, x_gather)
    x_all[held_part] = xcol[...]

    convert(1, up_hbm, down_hbm)
    convert(2, down_hbm, None)
    def pc(p, s):
        dst = send_order(s)

        @pl.when(dst != me)
        def _():
            piece_copy(p, dst).start()

    loop(pieces, lambda p: loop(fs_count, lambda s: pc(p, s)))

    wait_bytes(x_all.at[pl.ds(0, fs_count - 1)], x_sem.at[3])

    def project(m, out):
        act[m] = jnp.zeros_like(act[m])

        def body(k):
            g = jnp.where(k < half, near_source(k), far_source(k - half))

            @pl.when(g != me)
            def _():
                wait_bytes(out.at[g], recv_sem.at[m, g])

            x = x_all[g].astype(F32).reshape(tokens, width).astype(BF16)
            act[m] += jnp.dot(x, out[g], preferred_element_type=F32)

        loop(fs_count, body)

    project(0, gate_out)
    project(1, up_out)
    gate = act[0]
    hidden[...] = (gate / (1.0 + jnp.exp(-gate)) * act[1]).astype(BF16)

    def base_of(r):
        return jnp.where(lax.rem(r, 2) == 0, side, 1 - side) * half

    def finish(r):
        p = r // 2
        wait_bytes(rs_recv.at[r], rs_recv_sem.at[r])

        def add(s, acc):
            return acc + rs_recv[r, s].astype(F32)

        acc = lax.fori_loop(0, group - 1, add, part[r, index].astype(F32))
        total[r] = acc.astype(BF16)
        for q in range(pairs):
            tp = base_of(r) // share + q

            @pl.when(is_self(index, tp))
            def _(q=q):
                home[mine, p] = total[r, pl.ds(q * share, share)]

            @pl.when(jnp.logical_not(is_self(index, tp)))
            def _(q=q, tp=tp):
                home_copy(r, q, tp).start()

    def home_copy(r, q, tp):
        return pltpu.make_async_remote_copy(
            src_ref=total.at[r, pl.ds(q * share, share)], dst_ref=home.at[mine, r // 2],
            send_sem=home_send.at[r, q], recv_sem=home_recv.at[r // 2, mine],
            device_id={"fs": index, "tp": tp}, device_id_type=MESH,
        )

    def run_round(r):
        p = r // 2
        span = pl.ds(pl.multiple_of(p * rows, rows), rows)

        def item(k):
            g = jnp.where(lax.rem(r, 2) == 0, near_source(k), far_source(k))

            @pl.when(g != me)
            def _():
                wait_bytes(down_out.at[g, span], down_sem.at[p, g])

            out = lax.dot_general(
                hidden[...], down_out[g, span], (((1,), (1,)), ((), ())),
                preferred_element_type=F32,
            )
            part[r, :, g - base_of(r)] = out.reshape(fs_count, own, rows).astype(BF16)

        loop(half, item)

        def rs_send(s):
            i = lax.rem(index + 1 + s, fs_count)

            @pl.when(i != index)
            def _():
                fs, tp = plane_peer(i)
                slot = lax.rem(index + 2 * group - i - 1, group)
                pltpu.make_async_remote_copy(
                    src_ref=part.at[r, i], dst_ref=rs_recv.at[r, slot],
                    send_sem=rs_send_sem.at[r], recv_sem=rs_recv_sem.at[r],
                    device_id={"fs": fs, "tp": tp}, device_id_type=MESH,
                ).start()

        loop(fs_count, rs_send)

        @pl.when(jnp.logical_and(r > 0, index < fs_count))
        def _():
            finish(r - 1)

    turn[...] = jnp.zeros_like(turn)
    first, second = logits_ref[0:1], logits_ref[1:2]
    share_first = 1.0 / (1.0 + jnp.exp(second - first))
    share_second = 1.0 / (1.0 + jnp.exp(first - second))
    for e in range(experts):
        turn[e : e + 1, :own] = jnp.where(routes_ref[0:1] == e, share_first, 0.0) + jnp.where(
            routes_ref[1:2] == e, share_second, 0.0
        )
    weights = turn[...].T

    loop(rounds, run_round)

    @pl.when(index < fs_count)
    def _():
        finish(rounds - 1)

    for p in range(pieces):
        mixed = [jnp.zeros((own, rows), F32)] * share
        for e in range(experts):

            @pl.when(jnp.logical_not(is_self(*sender_of(e))))
            def _(e=e, p=p):
                wait_bytes(home.at[e, p], home_recv.at[p, e])

            for j in range(share):
                mixed[j] = mixed[j] + weights[:own, e : e + 1] * home[e, p, j].astype(F32)
        for j in range(share):
            column = j * width + p * rows
            mixed_out[:, column : column + rows] = mixed[j].astype(BF16)

    wait_bytes(xcol.at[pl.ds(0, fs_count - 1)], x_sem.at[0])
    wait_bytes(x_all.at[pl.ds(0, fs_count - 1)], x_sem.at[2])
    for m, held in enumerate((gate_send, up_send, down_send)):
        wait_bytes(held.at[pl.ds(0, fs_count - 1)], send_sem.at[m])

    def drain(r):
        @pl.when(index < fs_count)
        def _():
            wait_bytes(part.at[r, pl.ds(0, fs_count - 1)], rs_send_sem.at[r])
            for q in range(pairs):
                tp = base_of(r) // share + q

                @pl.when(jnp.logical_not(is_self(index, tp)))
                def _(q=q):
                    wait_bytes(total.at[r, pl.ds(q * share, share)], home_send.at[r, q])

        @pl.when(index >= fs_count)
        def _():
            wait_bytes(part.at[r], rs_send_sem.at[r])

    loop(rounds, drain)


def per_device(tokens, routes, route_logits, norm_gain, gate_weight, up_weight, down_weight):
    experts, width, columns = gate_weight.shape
    fs_count, tp_count = lax.axis_size("fs"), lax.axis_size("tp")
    spread = fs_count // experts
    block = columns // spread
    own, model = tokens.shape
    group = spread * tp_count
    half, share = fs_count // 2, fs_count // tp_count
    pieces = max(1, width // 128)
    rows = width // pieces
    rounds = 2 * pieces
    dma = pltpu.SemaphoreType.DMA
    vmem = pl.BlockSpec(memory_space=pltpu.VMEM)
    anywhere = pl.BlockSpec(memory_space=pl.ANY)
    pinned = [pltpu.VMEM((own, model // tp_count), BF16)]
    pinned += [pltpu.VMEM((fs_count, width, block), BF16)] * 3
    spare = [jax.ShapeDtypeStruct((fs_count, width, block), BF16)] * 2
    outs = pl.pallas_call(
        functools.partial(fused_kernel, fs_count, tp_count, experts, pieces),
        in_specs=[vmem] * 4 + [anywhere] * 3,
        out_specs=[vmem] * 4 + [anywhere] * 2,
        out_shape=pinned + spare,
        scratch_shapes=[
            pltpu.VMEM((2, width, block), F32),
            pltpu.VMEM((fs_count, width, block), BF16),
            pltpu.VMEM((2, width, block), BF16),
            pltpu.VMEM((8, 128), F32),
            pltpu.VMEM((width, 1), F32),
            pltpu.VMEM((share, own, width), BF16),
            pltpu.VMEM((fs_count, own, width), BF16),
            pltpu.VMEM((fs_count, fs_count, own, width), BF16),
            pltpu.VMEM((2, fs_count * own, block), F32),
            pltpu.VMEM((fs_count * own, block), BF16),
            pltpu.VMEM((rounds, fs_count, half, own, rows), BF16),
            pltpu.VMEM((rounds, group - 1, half, own, rows), BF16),
            pltpu.VMEM((rounds, half, own, rows), BF16),
            pltpu.VMEM((experts, pieces, share, own, rows), BF16),
            dma((2,)), dma((2,)), dma((3,)), dma((2, fs_count)), dma((pieces, fs_count)),
            dma((4,)), dma((rounds,)), dma((rounds,)), dma((rounds, tp_count // 2)),
            dma((pieces, experts)),
        ],
        compiler_params=pltpu.CompilerParams(
            collective_id=0, has_side_effects=True, vmem_limit_bytes=VMEM_BYTES - 6 * fs_count * width * block
        ),
    )(
        tokens, routes.T, route_logits.T, norm_gain.reshape(-1, 128),
        gate_weight, up_weight, down_weight,
    )
    mixed, *landings = pl.pallas_call(
        store_kernel,
        in_specs=[vmem] * 4,
        out_specs=[anywhere] * 4,
        out_shape=[jax.ShapeDtypeStruct(x.shape, x.dtype) for x in outs[:4]],
        scratch_shapes=[dma((4,))],
        compiler_params=pltpu.CompilerParams(vmem_limit_bytes=4 * 1024 * 1024),
    )(*outs[:4])
    return (mixed, *(x.reshape(1, fs_count * width, block) for x in landings))


def solution(mesh):
    in_specs = (
        P("fs", None),
        P("fs", None),
        P("fs", None),
        P("fs"),
        P(None, "fs", "tp"),
        P(None, "fs", "tp"),
        P(None, "fs", "tp"),
    )
    out_specs = (P("fs", "tp"), P("tp", None, "fs"), P("tp", None, "fs"), P("tp", None, "fs"))
    return jax.shard_map(
        per_device, mesh=mesh, in_specs=in_specs, out_specs=out_specs, check_vma=False
    )
```

```python
import functools

import jax
import jax.numpy as jnp
from jax import lax
from jax.experimental import pallas as pl
from jax.experimental.pallas import tpu as pltpu
from jax.sharding import PartitionSpec as P

MESH = pl.DeviceIdType.MESH
F32, BF16 = jnp.float32, jnp.bfloat16
VMEM_BYTES = 60 * 1024 * 1024


def wait_bytes(ref, sem):
    pltpu.make_async_copy(ref, ref, sem).wait()


def loop(count, body):
    def step(i, carry):
        body(i)
        return carry

    lax.fori_loop(0, count, step, 0)


def store_kernel(*refs):
    count = (len(refs) - 1) // 2
    held, out, sem = refs[:count], refs[count : 2 * count], refs[-1]
    pltpu.make_async_copy(held[0], out[0], sem.at[0]).start()
    for i in range(1, count):
        for g in range(held[i].shape[0]):
            pltpu.make_async_copy(held[i].at[g], out[i].at[g], sem.at[i]).start()
    for i in range(count):
        pltpu.make_async_copy(held[i], out[i], sem.at[i]).wait()


def fused_kernel(
    fs_count, tp_count, experts, pieces, relayed,
    tok_ref, routes_ref, logits_ref, gain_ref, gate_hbm, up_hbm, down_hbm,
    mixed_out, gate_out, up_out, down_out, up_send, down_send,
    stage, gate_send, packed, turn, gain_col,
    xown, xcol, x_all, act, hidden, part, rs_recv, total, home, relay, shares,
    load_sem, store_sem, send_sem, recv_sem, down_sem, x_sem,
    rs_send_sem, rs_recv_sem, home_send, home_recv, relay_send, relay_recv, share_sem,
):
    me, my_tp = lax.axis_index("fs"), lax.axis_index("tp")
    spread = fs_count // experts
    mine, inner = me // spread, lax.rem(me, spread)
    group = spread * tp_count
    index = inner * tp_count + my_tp
    half = fs_count // 2
    side = me // half
    share = fs_count // tp_count
    own, model = tok_ref.shape
    width, block = stage.shape[1], stage.shape[2]
    rows = width // pieces
    tokens = fs_count * own
    pairs = tp_count // 2
    rounds = 2 * pieces
    owner_fs, owner_tp = me // tp_count, lax.rem(me, tp_count)
    depth = experts // 2 - 1
    bridge = jnp.where(side == 0, depth, experts - 1 - depth)
    far_bridge = experts - 1 - bridge
    at_bridge = mine == bridge
    far_home = index // half != side
    home[...] = jnp.zeros_like(home)
    near_slots = pl.ds(0, half - 1)
    far_slots = pl.ds((1 - side) * half, half)

    def ranked(k):
        return jnp.where(side == 0, k, experts - 1 - k)

    def send_order(step):
        return lax.rem(me + half + step, fs_count)

    def near_source(k):
        return side * half + lax.rem(me + 2 * half - 1 - k, half)

    def far_source(k):
        return (1 - side) * half + lax.rem(me + half - k, half)

    def gather_peer(s):
        other = lax.rem(my_tp * share + lax.rem(inner, share) + s, fs_count)
        fs = mine * spread + (inner // share) * share + lax.rem(other, share)
        return fs, other // share

    def plane_peer(i):
        return mine * spread + i // tp_count, lax.rem(i, tp_count)

    barrier = pltpu.get_barrier_semaphore()

    def signal(fs, tp):
        pl.semaphore_signal(
            barrier, inc=1, device_id={"fs": fs, "tp": tp}, device_id_type=MESH
        )

    def load(hbm, step, slot):
        dst = send_order(step)
        column = pl.multiple_of(lax.rem(dst, spread) * block, block)
        return pltpu.make_async_copy(
            hbm.at[dst // spread, :, pl.ds(column, block)], stage.at[slot], load_sem.at[slot]
        )

    load(gate_hbm, 0, 0).start()
    loop(fs_count - 1, lambda s: signal(lax.rem(me + 1 + s, fs_count), my_tp))

    def greet(s):
        fs, tp = plane_peer(lax.rem(index + 1 + s, group))
        signal(fs, tp)

    loop(group - 1, greet)

    def sender_of(e):
        return e * spread + owner_fs, owner_tp

    def is_self(fs, tp):
        return jnp.logical_and(fs == me, tp == my_tp)

    for e in range(experts):
        fs, tp = sender_of(e)

        @pl.when(jnp.logical_not(is_self(fs, tp)))
        def _(fs=fs, tp=tp):
            signal(fs, tp)

    turn[...] = jnp.zeros_like(turn)
    turn[: gain_ref.shape[0]] = gain_ref[...]
    turned = turn[...].T
    for q in range(width // 128):
        gain_col[q * 128 : (q + 1) * 128] = turned[:, q : q + 1]

    tok = tok_ref[...].astype(F32)
    scale = lax.rsqrt(jnp.mean(tok * tok, axis=1, keepdims=True) + 1e-05)
    for j in range(share):
        column = pl.multiple_of((my_tp * share + j) * width, width)
        cols = tok_ref[:, pl.ds(column, width)].astype(F32)
        xown[j] = (cols * scale).astype(BF16)
    xcol[me] = xown[lax.rem(inner, share)]

    homes = jnp.where(index < fs_count, tp_count, 0) - jnp.where(index == me, 1, 0)
    pl.semaphore_wait(barrier, fs_count + group - 2 + homes)

    def x_send(dst):
        pltpu.make_async_remote_copy(
            src_ref=xown.at[lax.rem(lax.rem(dst, spread), share)], dst_ref=xcol.at[me],
            send_sem=x_sem.at[0], recv_sem=x_sem.at[1], device_id={"fs": dst},
            device_id_type=MESH,
        ).start()

    loop(spread, lambda h: x_send(far_bridge * spread + lax.rem(inner + h, spread)))
    loop(half - 1, lambda s: x_send(side * half + lax.rem(me + 1 + s, half)))

    def shares_copy(fs):
        return pltpu.make_async_remote_copy(
            src_ref=turn, dst_ref=shares, send_sem=share_sem.at[0], recv_sem=share_sem.at[1],
            device_id={"fs": fs}, device_id_type=MESH,
        )

    def for_planes(action):
        for e in range(experts):
            fs = e * spread + owner_fs

            @pl.when(jnp.logical_and(my_tp == owner_tp, fs != me))
            def _(fs=fs):
                action(fs)

    turn[...] = jnp.zeros_like(turn)
    first, second = logits_ref[0:1], logits_ref[1:2]
    share_first = 1.0 / (1.0 + jnp.exp(second - first))
    share_second = 1.0 / (1.0 + jnp.exp(first - second))
    for e in range(experts):
        turn[e : e + 1, :own] = jnp.where(routes_ref[0:1] == e, share_first, 0.0) + jnp.where(
            routes_ref[1:2] == e, share_second, 0.0
        )
    for_planes(lambda fs: shares_copy(fs).start())

    @pl.when(index == me)
    def _():
        shares[...] = turn[...]

    def block_copy(m, held, out, dst):
        return pltpu.make_async_remote_copy(
            src_ref=held.at[dst], dst_ref=out.at[me], send_sem=send_sem.at[m],
            recv_sem=recv_sem.at[m, me], device_id={"fs": dst}, device_id_type=MESH,
        )

    def piece_copy(p, dst):
        span = pl.ds(pl.multiple_of(p * rows, rows), rows)
        return pltpu.make_async_remote_copy(
            src_ref=down_send.at[dst, span], dst_ref=down_out.at[me, span],
            send_sem=send_sem.at[2], recv_sem=down_sem.at[p, me], device_id={"fs": dst},
            device_id_type=MESH,
        )

    def convert(m, hbm, following):
        def body(step):
            slot = lax.rem(m * fs_count + step, 2)
            dst = send_order(step)

            @pl.when(step + 1 < fs_count)
            def _():
                load(hbm, step + 1, 1 - slot).start()

            if following is not None:

                @pl.when(step + 1 == fs_count)
                def _():
                    load(following, 0, 1 - slot).start()

            load(hbm, step, slot).wait()
            held, out = ((gate_send, gate_out), (up_send, up_out), (down_send, down_out))[m]
            block_f32 = stage[slot]
            if m < 2:
                block_f32 = block_f32 * gain_col[...]
            rounded = block_f32.astype(BF16)

            @pl.when(dst == me)
            def _():
                out[me] = rounded

            @pl.when(dst != me)
            def _():
                if m == 0:
                    held[dst] = rounded
                    block_copy(m, held, out, dst).start()
                else:
                    packed[slot] = rounded
                    store(held, step).start()

            if m > 0:

                @pl.when(jnp.logical_and(step > 0, send_order(step - 1) != me))
                def _():
                    stored(m, held, out, step - 1)

        def store(held, step):
            slot = lax.rem(m * fs_count + step, 2)
            return pltpu.make_async_copy(
                packed.at[slot], held.at[send_order(step)], store_sem.at[slot]
            )

        def stored(m, held, out, step):
            store(held, step).wait()
            if m == 1:
                block_copy(m, held, out, send_order(step)).start()

        loop(fs_count, body)
        if m > 0:
            held, out = ((up_send, up_out), (down_send, down_out))[m - 1]

            @pl.when(send_order(fs_count - 1) != me)
            def _():
                stored(m, held, out, fs_count - 1)

    convert(0, gate_hbm, up_hbm)

    def x_forward(k):
        return pltpu.make_async_remote_copy(
            src_ref=xcol.at[far_slots], dst_ref=xcol.at[far_slots], send_sem=x_sem.at[4],
            recv_sem=x_sem.at[5], device_id={"fs": ranked(k) * spread + inner},
            device_id_type=MESH,
        )

    @pl.when(at_bridge)
    def _():
        wait_bytes(xcol.at[pl.ds(0, fs_count - 1)], x_sem.at[1])
        loop(depth, lambda k: x_forward(k).start())

    @pl.when(jnp.logical_not(at_bridge))
    def _():
        wait_bytes(xcol.at[near_slots], x_sem.at[1])
        wait_bytes(xcol.at[far_slots], x_sem.at[5])

    held_part = my_tp * share + lax.rem(inner, share)

    def x_gather(s):
        fs, tp = gather_peer(s + 1)
        pltpu.make_async_remote_copy(
            src_ref=xcol, dst_ref=x_all.at[held_part], send_sem=x_sem.at[2],
            recv_sem=x_sem.at[3], device_id={"fs": fs, "tp": tp}, device_id_type=MESH,
        ).start()

    loop(fs_count - 1, x_gather)
    x_all[held_part] = xcol[...]

    convert(1, up_hbm, down_hbm)
    convert(2, down_hbm, None)
    def pc(p, s):
        dst = send_order(s)

        @pl.when(dst != me)
        def _():
            piece_copy(p, dst).start()

    loop(pieces, lambda p: loop(fs_count, lambda s: pc(p, s)))

    wait_bytes(x_all.at[pl.ds(0, fs_count - 1)], x_sem.at[3])

    def project(m, out):
        act[m] = jnp.zeros_like(act[m])

        def body(k):
            g = jnp.where(k < half, near_source(k), far_source(k - half))

            @pl.when(g != me)
            def _():
                wait_bytes(out.at[g], recv_sem.at[m, g])

            x = x_all[g].astype(F32).reshape(tokens, width).astype(BF16)
            act[m] += jnp.dot(x, out[g], preferred_element_type=F32)

        loop(fs_count, body)

    project(0, gate_out)
    project(1, up_out)
    gate = act[0]
    hidden[...] = (gate / (1.0 + jnp.exp(-gate)) * act[1]).astype(BF16)

    def base_of(r):
        return jnp.where(lax.rem(r, 2) == 0, side, 1 - side) * half

    def finish(r):
        wait_bytes(rs_recv.at[r], rs_recv_sem.at[r])

        def add(s, acc):
            return acc + rs_recv[r, s].astype(F32)

        acc = lax.fori_loop(0, group - 1, add, part[r, index].astype(F32))
        columns = shares[...].T
        lanes = lax.broadcasted_iota(jnp.int32, columns.shape, 1)
        scale = jnp.sum(jnp.where(lanes == mine, columns, 0.0), axis=1, keepdims=True)
        total[r] = (acc * scale[:own][None]).astype(BF16)
        if relayed == 0:
            send_home(r)
            return
        detour = detours(r)

        @pl.when(jnp.logical_and(detour, jnp.logical_not(at_bridge)))
        def _():
            relay_copy(r).start()

        @pl.when(jnp.logical_not(detour))
        def _():
            send_home(r)

    def detours(r):
        return jnp.logical_and(far_home, r < relayed)

    def relay_copy(r):
        return pltpu.make_async_remote_copy(
            src_ref=total.at[r], dst_ref=relay.at[r, jnp.where(side == 0, mine, experts - 1 - mine)],
            send_sem=relay_send.at[r], recv_sem=relay_recv.at[r],
            device_id={"fs": bridge * spread + inner}, device_id_type=MESH,
        )

    def cross(r):
        wait_bytes(relay.at[r], relay_recv.at[r])
        acc = total[r].astype(F32)
        for k in range(depth):
            acc = acc + relay[r, k].astype(F32)
        total[r] = acc.astype(BF16)
        send_home(r)

    def send_home(r):
        p = r // 2
        for q in range(pairs):
            tp = base_of(r) // share + q

            @pl.when(is_self(index, tp))
            def _(q=q):
                home[mine, p] = total[r, pl.ds(q * share, share)]

            @pl.when(jnp.logical_not(is_self(index, tp)))
            def _(q=q, tp=tp):
                home_copy(r, q, tp).start()

    def home_copy(r, q, tp):
        return pltpu.make_async_remote_copy(
            src_ref=total.at[r, pl.ds(q * share, share)], dst_ref=home.at[mine, r // 2],
            send_sem=home_send.at[r, q], recv_sem=home_recv.at[r // 2, mine],
            device_id={"fs": index, "tp": tp}, device_id_type=MESH,
        )

    def run_round(r):
        p = r // 2
        span = pl.ds(pl.multiple_of(p * rows, rows), rows)

        def item(k):
            g = jnp.where(lax.rem(r, 2) == 0, near_source(k), far_source(k))

            @pl.when(g != me)
            def _():
                wait_bytes(down_out.at[g, span], down_sem.at[p, g])

            out = lax.dot_general(
                hidden[...], down_out[g, span], (((1,), (1,)), ((), ())),
                preferred_element_type=F32,
            )
            part[r, :, g - base_of(r)] = out.reshape(fs_count, own, rows).astype(BF16)

        loop(half, item)

        def rs_send(s):
            i = lax.rem(index + 1 + s, fs_count)

            @pl.when(i != index)
            def _():
                fs, tp = plane_peer(i)
                slot = lax.rem(index + 2 * group - i - 1, group)
                pltpu.make_async_remote_copy(
                    src_ref=part.at[r, i], dst_ref=rs_recv.at[r, slot],
                    send_sem=rs_send_sem.at[r], recv_sem=rs_recv_sem.at[r],
                    device_id={"fs": fs, "tp": tp}, device_id_type=MESH,
                ).start()

        loop(fs_count, rs_send)

        @pl.when(jnp.logical_and(r > 0, index < fs_count))
        def _():
            finish(r - 1)

    @pl.when(jnp.logical_and(index < fs_count, index != me))
    def _():
        wait_bytes(shares, share_sem.at[1])

    loop(rounds, run_round)

    @pl.when(index < fs_count)
    def _():
        if relayed > 0:

            @pl.when(jnp.logical_and(far_home, at_bridge))
            def _():
                loop(relayed, cross)

        finish(rounds - 1)

    for p in range(pieces):
        mixed = [jnp.zeros((own, rows), F32)] * share
        for e in range(experts):

            sent = jnp.logical_not(is_self(*sender_of(e)))
            if relayed > 0:
                apart = jnp.where(my_tp // pairs == e // (depth + 1), 0, 1)
                skipped = jnp.logical_and(side != e // (depth + 1), 2 * p + apart < relayed)
                sent = jnp.logical_and(
                    sent, jnp.logical_or(jnp.logical_not(skipped), e == far_bridge)
                )

            @pl.when(sent)
            def _(e=e, p=p):
                wait_bytes(home.at[e, p], home_recv.at[p, e])

            for j in range(share):
                mixed[j] = mixed[j] + home[e, p, j].astype(F32)
        for j in range(share):
            column = j * width + p * rows
            mixed_out[:, column : column + rows] = mixed[j].astype(BF16)

    wait_bytes(xcol.at[pl.ds(0, spread + half - 1)], x_sem.at[0])
    for_planes(lambda fs: shares_copy(fs).wait_send())

    @pl.when(at_bridge)
    def _():
        loop(depth, lambda k: x_forward(k).wait_send())

    wait_bytes(x_all.at[pl.ds(0, fs_count - 1)], x_sem.at[2])
    for m, held in enumerate((gate_send, up_send, down_send)):
        wait_bytes(held.at[pl.ds(0, fs_count - 1)], send_sem.at[m])

    def drain(r):
        @pl.when(index < fs_count)
        def _():
            wait_bytes(part.at[r, pl.ds(0, fs_count - 1)], rs_send_sem.at[r])
            passed = jnp.logical_and(detours(r), jnp.logical_not(at_bridge))

            @pl.when(passed)
            def _():
                relay_copy(r).wait_send()

            for q in range(pairs):
                tp = base_of(r) // share + q

                @pl.when(jnp.logical_not(jnp.logical_or(passed, is_self(index, tp))))
                def _(q=q):
                    wait_bytes(total.at[r, pl.ds(q * share, share)], home_send.at[r, q])

        @pl.when(index >= fs_count)
        def _():
            wait_bytes(part.at[r], rs_send_sem.at[r])

    loop(rounds, drain)


def per_device(tokens, routes, route_logits, norm_gain, gate_weight, up_weight, down_weight):
    experts, width, columns = gate_weight.shape
    fs_count, tp_count = lax.axis_size("fs"), lax.axis_size("tp")
    spread = fs_count // experts
    block = columns // spread
    own, model = tokens.shape
    group = spread * tp_count
    half, share = fs_count // 2, fs_count // tp_count
    pieces = max(1, width // 128)
    rows = width // pieces
    rounds = 2 * pieces
    relayed = max(0, rounds - 2)
    depth = max(1, experts // 2 - 1)
    dma = pltpu.SemaphoreType.DMA
    vmem = pl.BlockSpec(memory_space=pltpu.VMEM)
    anywhere = pl.BlockSpec(memory_space=pl.ANY)
    pinned = [pltpu.VMEM((own, model // tp_count), BF16)]
    pinned += [pltpu.VMEM((fs_count, width, block), BF16)] * 3
    spare = [jax.ShapeDtypeStruct((fs_count, width, block), BF16)] * 2
    outs = pl.pallas_call(
        functools.partial(fused_kernel, fs_count, tp_count, experts, pieces, relayed),
        in_specs=[vmem] * 4 + [anywhere] * 3,
        out_specs=[vmem] * 4 + [anywhere] * 2,
        out_shape=pinned + spare,
        scratch_shapes=[
            pltpu.VMEM((2, width, block), F32),
            pltpu.VMEM((fs_count, width, block), BF16),
            pltpu.VMEM((2, width, block), BF16),
            pltpu.VMEM((8, 128), F32),
            pltpu.VMEM((width, 1), F32),
            pltpu.VMEM((share, own, width), BF16),
            pltpu.VMEM((fs_count, own, width), BF16),
            pltpu.VMEM((fs_count, fs_count, own, width), BF16),
            pltpu.VMEM((2, fs_count * own, block), F32),
            pltpu.VMEM((fs_count * own, block), BF16),
            pltpu.VMEM((rounds, fs_count, half, own, rows), BF16),
            pltpu.VMEM((rounds, group - 1, half, own, rows), BF16),
            pltpu.VMEM((rounds, half, own, rows), BF16),
            pltpu.VMEM((experts, pieces, share, own, rows), BF16),
            pltpu.VMEM((max(1, relayed), depth, half, own, rows), BF16),
            pltpu.VMEM((8, 128), F32),
            dma((2,)), dma((2,)), dma((3,)), dma((2, fs_count)), dma((pieces, fs_count)),
            dma((6,)), dma((rounds,)), dma((rounds,)), dma((rounds, tp_count // 2)),
            dma((pieces, experts)), dma((max(1, relayed),)), dma((max(1, relayed),)), dma((2,)),
        ],
        compiler_params=pltpu.CompilerParams(
            collective_id=0, has_side_effects=True, vmem_limit_bytes=VMEM_BYTES - 6 * fs_count * width * block
        ),
    )(
        tokens, routes.T, route_logits.T, norm_gain.reshape(-1, 128),
        gate_weight, up_weight, down_weight,
    )
    mixed, *landings = pl.pallas_call(
        store_kernel,
        in_specs=[vmem] * 4,
        out_specs=[anywhere] * 4,
        out_shape=[jax.ShapeDtypeStruct(x.shape, x.dtype) for x in outs[:4]],
        scratch_shapes=[dma((4,))],
        compiler_params=pltpu.CompilerParams(vmem_limit_bytes=4 * 1024 * 1024),
    )(*outs[:4])
    return (mixed, *(x.reshape(1, fs_count * width, block) for x in landings))


def solution(mesh):
    in_specs = (
        P("fs", None),
        P("fs", None),
        P("fs", None),
        P("fs"),
        P(None, "fs", "tp"),
        P(None, "fs", "tp"),
        P(None, "fs", "tp"),
    )
    out_specs = (P("fs", "tp"), P("tp", None, "fs"), P("tp", None, "fs"), P("tp", None, "fs"))
    return jax.shard_map(
        per_device, mesh=mesh, in_specs=in_specs, out_specs=out_specs, check_vma=False
    )
```

```python
import functools

import jax
import jax.numpy as jnp
from jax import lax
from jax.experimental import pallas as pl
from jax.experimental.pallas import tpu as pltpu
from jax.sharding import PartitionSpec as P

MESH = pl.DeviceIdType.MESH
F32, BF16 = jnp.float32, jnp.bfloat16
VMEM_BYTES = 60 * 1024 * 1024


def wait_bytes(ref, sem):
    pltpu.make_async_copy(ref, ref, sem).wait()


def loop(count, body):
    def step(i, carry):
        body(i)
        return carry

    lax.fori_loop(0, count, step, 0)


def store_kernel(*refs):
    count = (len(refs) - 1) // 2
    held, out, sem = refs[:count], refs[count : 2 * count], refs[-1]
    pltpu.make_async_copy(held[0], out[0], sem.at[0]).start()
    for i in range(1, count):
        for g in range(held[i].shape[0]):
            pltpu.make_async_copy(held[i].at[g], out[i].at[g], sem.at[i]).start()
    for i in range(count):
        pltpu.make_async_copy(held[i], out[i], sem.at[i]).wait()


def fused_kernel(
    fs_count, tp_count, experts, pieces, relayed,
    tok_hbm, routes_hbm, logits_hbm, gain_hbm, gate_hbm, up_hbm, down_hbm,
    mixed_out, gate_out, up_out, down_out, up_send, down_send,
    tok_ref, routes_ref, logits_ref, gain_ref, stage, gate_send, packed, turn, gain_col,
    share_col,
    xown, xcol, x_all, act, hidden, part, rs_recv, total, home, relay, shares,
    load_sem, store_sem, send_sem, recv_sem, down_sem, x_sem,
    rs_send_sem, rs_recv_sem, home_send, home_recv, relay_send, relay_recv, share_sem, small_sem,
):
    me, my_tp = lax.axis_index("fs"), lax.axis_index("tp")
    spread = fs_count // experts
    mine, inner = me // spread, lax.rem(me, spread)
    group = spread * tp_count
    index = inner * tp_count + my_tp
    half = fs_count // 2
    side = me // half
    share = fs_count // tp_count
    own, model = tok_ref.shape
    width, block = stage.shape[1], stage.shape[2]
    rows = width // pieces
    tokens = fs_count * own
    pairs = tp_count // 2
    rounds = 2 * pieces
    planes = experts // 2

    def seat(z):
        return lax.rem(z, planes) * 2 + z // planes

    handled = (lax.rem(my_tp, 2) * planes + my_tp // 2) * spread + inner
    handles = my_tp < experts
    own_home = jnp.logical_and(handles, handled == me)
    depth = experts // 2 - 1
    bridge = jnp.where(side == 0, depth, experts - 1 - depth)
    far_bridge = experts - 1 - bridge
    at_bridge = mine == bridge
    far_home = handled // half != side
    near_slots = pl.ds(0, half - 1)
    far_slots = pl.ds((1 - side) * half, half)

    def ranked(k):
        return jnp.where(side == 0, k, experts - 1 - k)

    def send_order(step):
        return lax.rem(me + half + step, fs_count)

    def near_source(k):
        return side * half + lax.rem(me + 2 * half - 1 - k, half)

    def far_source(k):
        return (1 - side) * half + lax.rem(me + half - k, half)

    def gather_peer(s):
        other = lax.rem(my_tp * share + lax.rem(inner, share) + s, fs_count)
        fs = mine * spread + (inner // share) * share + lax.rem(other, share)
        return fs, other // share

    def plane_peer(i):
        return mine * spread + lax.rem(i, spread), seat(i // spread)

    small = [
        pltpu.make_async_copy(hbm, ref, small_sem.at[i])
        for i, (hbm, ref) in enumerate(
            (
                (gain_hbm, gain_ref), (tok_hbm, tok_ref), (routes_hbm, routes_ref),
                (logits_hbm, logits_ref),
            )
        )
    ]
    barrier = pltpu.get_barrier_semaphore()

    def signal(fs, tp):
        pl.semaphore_signal(
            barrier, inc=1, device_id={"fs": fs, "tp": tp}, device_id_type=MESH
        )

    def load(hbm, step, slot):
        dst = send_order(step)
        column = pl.multiple_of(lax.rem(dst, spread) * block, block)
        return pltpu.make_async_copy(
            hbm.at[dst // spread, :, pl.ds(column, block)], stage.at[slot], load_sem.at[slot]
        )

    small[0].start()
    load(gate_hbm, 0, 0).start()
    for copy in small[1:]:
        copy.start()
    home[...] = jnp.zeros_like(home)
    loop(fs_count - 1, lambda s: signal(lax.rem(me + 1 + s, fs_count), my_tp))

    def greet(s):
        other = lax.rem(index + 1 + s, group)
        signal(mine * spread + other // tp_count, lax.rem(other, tp_count))

    loop(group - 1, greet)

    def sender_of(e):
        return e * spread + inner, seat(mine)

    def is_self(fs, tp):
        return jnp.logical_and(fs == me, tp == my_tp)

    for e in range(experts):
        fs, tp = sender_of(e)

        @pl.when(jnp.logical_not(is_self(fs, tp)))
        def _(fs=fs, tp=tp):
            signal(fs, tp)

    turn[...] = jnp.zeros_like(turn)
    small[0].wait()
    turn[: gain_ref.shape[0]] = gain_ref[...]
    turned = turn[...].T
    for q in range(width // 128):
        gain_col[q * 128 : (q + 1) * 128] = turned[:, q : q + 1]

    load(gate_hbm, 0, 0).wait()
    load(gate_hbm, 1, 1).start()
    gate_send[send_order(0)] = (stage[0] * gain_col[...]).astype(BF16)
    for copy in small[1:]:
        copy.wait()
    tok = tok_ref[...].astype(F32)
    scale = lax.rsqrt(jnp.mean(tok * tok, axis=1, keepdims=True) + 1e-05)
    for j in range(share):
        column = pl.multiple_of((my_tp * share + j) * width, width)
        cols = tok_ref[:, pl.ds(column, width)].astype(F32)
        xown[j] = (cols * scale).astype(BF16)
    xcol[me] = xown[lax.rem(inner, share)]

    homes = jnp.where(handles, tp_count, 0) - jnp.where(own_home, 1, 0)
    pl.semaphore_wait(barrier, fs_count + group - 2 + homes)

    def block_copy(m, held, out, dst):
        return pltpu.make_async_remote_copy(
            src_ref=held.at[dst], dst_ref=out.at[me], send_sem=send_sem.at[m],
            recv_sem=recv_sem.at[m, me], device_id={"fs": dst}, device_id_type=MESH,
        )

    block_copy(0, gate_send, gate_out, send_order(0)).start()

    def x_send(dst):
        pltpu.make_async_remote_copy(
            src_ref=xown.at[lax.rem(lax.rem(dst, spread), share)], dst_ref=xcol.at[me],
            send_sem=x_sem.at[0], recv_sem=x_sem.at[1], device_id={"fs": dst},
            device_id_type=MESH,
        ).start()

    loop(spread, lambda h: x_send(far_bridge * spread + lax.rem(inner + h, spread)))
    loop(half - 1, lambda s: x_send(side * half + lax.rem(me + 1 + s, half)))

    def shares_copy(fs):
        return pltpu.make_async_remote_copy(
            src_ref=turn, dst_ref=shares, send_sem=share_sem.at[0], recv_sem=share_sem.at[1],
            device_id={"fs": fs}, device_id_type=MESH,
        )

    def for_planes(action):
        for e in range(experts):
            fs = e * spread + inner

            @pl.when(jnp.logical_and(my_tp == seat(mine), fs != me))
            def _(fs=fs):
                action(fs)

    turn[...] = jnp.zeros_like(turn)
    first, second = logits_ref[0:1], logits_ref[1:2]
    share_first = 1.0 / (1.0 + jnp.exp(second - first))
    share_second = 1.0 / (1.0 + jnp.exp(first - second))
    for e in range(experts):
        turn[e : e + 1, :own] = jnp.where(routes_ref[0:1] == e, share_first, 0.0) + jnp.where(
            routes_ref[1:2] == e, share_second, 0.0
        )
    for_planes(lambda fs: shares_copy(fs).start())

    @pl.when(own_home)
    def _():
        shares[...] = turn[...]

    def piece_copy(p, dst):
        span = pl.ds(pl.multiple_of(p * rows, rows), rows)
        return pltpu.make_async_remote_copy(
            src_ref=down_send.at[dst, span], dst_ref=down_out.at[me, span],
            send_sem=send_sem.at[2], recv_sem=down_sem.at[p, me], device_id={"fs": dst},
            device_id_type=MESH,
        )

    def convert(m, hbm, following):
        begin = 1 if m == 0 else 0

        def body(i):
            step = i + begin
            slot = lax.rem(m * fs_count + step, 2)
            dst = send_order(step)

            @pl.when(step + 1 < fs_count)
            def _():
                load(hbm, step + 1, 1 - slot).start()

            if following is not None:

                @pl.when(step + 1 == fs_count)
                def _():
                    load(following, 0, 1 - slot).start()

            load(hbm, step, slot).wait()
            held, out = ((gate_send, gate_out), (up_send, up_out), (down_send, down_out))[m]
            block_f32 = stage[slot]
            if m < 2:
                block_f32 = block_f32 * gain_col[...]
            rounded = block_f32.astype(BF16)

            @pl.when(dst == me)
            def _():
                out[me] = rounded

            @pl.when(dst != me)
            def _():
                if m == 0:
                    held[dst] = rounded
                    block_copy(m, held, out, dst).start()
                else:
                    packed[slot] = rounded
                    store(held, step).start()

            if m > 0:

                @pl.when(jnp.logical_and(step > 0, send_order(step - 1) != me))
                def _():
                    stored(m, held, out, step - 1)

        def store(held, step):
            slot = lax.rem(m * fs_count + step, 2)
            return pltpu.make_async_copy(
                packed.at[slot], held.at[send_order(step)], store_sem.at[slot]
            )

        def stored(m, held, out, step):
            store(held, step).wait()
            if m == 1:
                block_copy(m, held, out, send_order(step)).start()

        loop(fs_count - begin, body)
        if m > 0:
            held, out = ((up_send, up_out), (down_send, down_out))[m - 1]

            @pl.when(send_order(fs_count - 1) != me)
            def _():
                stored(m, held, out, fs_count - 1)

    convert(0, gate_hbm, up_hbm)

    def x_forward(k):
        return pltpu.make_async_remote_copy(
            src_ref=xcol.at[far_slots], dst_ref=xcol.at[far_slots], send_sem=x_sem.at[4],
            recv_sem=x_sem.at[5], device_id={"fs": ranked(k) * spread + inner},
            device_id_type=MESH,
        )

    @pl.when(at_bridge)
    def _():
        wait_bytes(xcol.at[pl.ds(0, fs_count - 1)], x_sem.at[1])
        loop(depth, lambda k: x_forward(k).start())

    @pl.when(jnp.logical_not(at_bridge))
    def _():
        wait_bytes(xcol.at[near_slots], x_sem.at[1])
        wait_bytes(xcol.at[far_slots], x_sem.at[5])

    held_part = my_tp * share + lax.rem(inner, share)

    def x_gather(s):
        fs, tp = gather_peer(s + 1)
        pltpu.make_async_remote_copy(
            src_ref=xcol, dst_ref=x_all.at[held_part], send_sem=x_sem.at[2],
            recv_sem=x_sem.at[3], device_id={"fs": fs, "tp": tp}, device_id_type=MESH,
        ).start()

    loop(fs_count - 1, x_gather)
    x_all[held_part] = xcol[...]

    convert(1, up_hbm, down_hbm)
    convert(2, down_hbm, None)
    def pc(p, s):
        dst = send_order(s)

        @pl.when(dst != me)
        def _():
            piece_copy(p, dst).start()

    loop(pieces, lambda p: loop(fs_count, lambda s: pc(p, s)))

    wait_bytes(x_all.at[pl.ds(0, fs_count - 1)], x_sem.at[3])

    def project(m, out):
        act[m] = jnp.zeros_like(act[m])

        def body(k):
            g = jnp.where(k < half, near_source(k), far_source(k - half))

            @pl.when(g != me)
            def _():
                wait_bytes(out.at[g], recv_sem.at[m, g])

            x = x_all[g].astype(F32).reshape(tokens, width).astype(BF16)
            act[m] += jnp.dot(x, out[g], preferred_element_type=F32)

        loop(fs_count, body)

    project(0, gate_out)
    project(1, up_out)
    gate = act[0]
    hidden[...] = (gate / (1.0 + jnp.exp(-gate)) * act[1]).astype(BF16)

    def base_of(r):
        return jnp.where(lax.rem(r, 2) == 0, side, 1 - side) * half

    def finish(r):
        wait_bytes(rs_recv.at[r], rs_recv_sem.at[r])

        def add(s, acc):
            return acc + rs_recv[r, s].astype(F32)

        acc = lax.fori_loop(0, group - 1, add, part[r, handled].astype(F32))
        total[r] = (acc * share_col[...][None]).astype(BF16)
        if relayed == 0:
            send_home(r)
            return
        detour = detours(r)

        @pl.when(jnp.logical_and(detour, jnp.logical_not(at_bridge)))
        def _():
            relay_copy(r).start()

        @pl.when(jnp.logical_not(detour))
        def _():
            send_home(r)

    def detours(r):
        return jnp.logical_and(far_home, r < relayed)

    def relay_copy(r):
        return pltpu.make_async_remote_copy(
            src_ref=total.at[r], dst_ref=relay.at[r, jnp.where(side == 0, mine, experts - 1 - mine)],
            send_sem=relay_send.at[r], recv_sem=relay_recv.at[r],
            device_id={"fs": bridge * spread + inner}, device_id_type=MESH,
        )

    def cross(r):
        wait_bytes(relay.at[r], relay_recv.at[r])
        acc = total[r].astype(F32)
        for k in range(depth):
            acc = acc + relay[r, k].astype(F32)
        total[r] = acc.astype(BF16)
        send_home(r)

    def send_home(r):
        p = r // 2
        for q in range(pairs):
            tp = base_of(r) // share + q

            @pl.when(is_self(handled, tp))
            def _(q=q):
                home[mine, p] = total[r, q]

            @pl.when(jnp.logical_not(is_self(handled, tp)))
            def _(q=q, tp=tp):
                home_copy(r, q, tp).start()

    def home_copy(r, q, tp):
        return pltpu.make_async_remote_copy(
            src_ref=total.at[r, q], dst_ref=home.at[mine, r // 2],
            send_sem=home_send.at[r, q], recv_sem=home_recv.at[r // 2, mine],
            device_id={"fs": handled, "tp": tp}, device_id_type=MESH,
        )

    column = lax.rem(me, half)
    first_cut = jnp.where(jnp.logical_or(column < share // 2, column >= half - share // 2), 1, 0)

    def run_round(r):
        p = r // 2
        span = pl.ds(pl.multiple_of(p * rows, rows), rows)

        def project_back(g):
            @pl.when(g != me)
            def _():
                wait_bytes(down_out.at[g, span], down_sem.at[p, g])

            out = lax.dot_general(
                hidden[...], down_out[g, span], (((1,), (1,)), ((), ())),
                preferred_element_type=F32,
            )
            return out.reshape(fs_count, own, rows)

        def cut(k):
            q = lax.rem(k + first_cut, pairs)
            base = base_of(r) + q * share
            outs = [project_back(base + j) for j in range(share)]
            part[r, :, q] = jnp.concatenate(outs, axis=1).astype(BF16)

            def rs_send(s):
                i = lax.rem(me + 1 + s, fs_count)
                fs, tp = plane_peer(i)

                @pl.when(jnp.logical_not(is_self(fs, tp)))
                def _():
                    place = lax.rem(i, spread) * tp_count + tp
                    slot = lax.rem(index + 2 * group - place - 1, group)
                    pltpu.make_async_remote_copy(
                        src_ref=part.at[r, i, q], dst_ref=rs_recv.at[r, slot, q],
                        send_sem=rs_send_sem.at[r], recv_sem=rs_recv_sem.at[r],
                        device_id={"fs": fs, "tp": tp}, device_id_type=MESH,
                    ).start()

            loop(fs_count, rs_send)

        loop(pairs, cut)

        @pl.when(jnp.logical_and(r > 0, handles))
        def _():
            finish(r - 1)

    @pl.when(jnp.logical_and(handles, handled != me))
    def _():
        wait_bytes(shares, share_sem.at[1])

    @pl.when(handles)
    def _():
        columns = shares[...].T
        lanes = lax.broadcasted_iota(jnp.int32, columns.shape, 1)
        scale = jnp.sum(jnp.where(lanes == mine, columns, 0.0), axis=1, keepdims=True)
        for j in range(share):
            share_col[j * own : (j + 1) * own] = scale[:own]

    loop(rounds, run_round)

    @pl.when(handles)
    def _():
        if relayed > 0:

            @pl.when(jnp.logical_and(far_home, at_bridge))
            def _():
                loop(relayed, cross)

        finish(rounds - 1)

    for p in range(pieces):
        mixed = [jnp.zeros((own, rows), F32)] * share
        for e in range(experts):

            sent = jnp.logical_not(is_self(*sender_of(e)))
            if relayed > 0:
                apart = jnp.where(my_tp // pairs == e // (depth + 1), 0, 1)
                skipped = jnp.logical_and(side != e // (depth + 1), 2 * p + apart < relayed)
                sent = jnp.logical_and(
                    sent, jnp.logical_or(jnp.logical_not(skipped), e == far_bridge)
                )

            @pl.when(sent)
            def _(e=e, p=p):
                wait_bytes(home.at[e, p], home_recv.at[p, e])

            landed = home[e, p].astype(F32)
            for j in range(share):
                mixed[j] = mixed[j] + landed[j * own : (j + 1) * own]
        for j in range(share):
            column = j * width + p * rows
            mixed_out[:, column : column + rows] = mixed[j].astype(BF16)

    wait_bytes(xcol.at[pl.ds(0, spread + half - 1)], x_sem.at[0])
    for_planes(lambda fs: shares_copy(fs).wait_send())

    @pl.when(at_bridge)
    def _():
        loop(depth, lambda k: x_forward(k).wait_send())

    wait_bytes(x_all.at[pl.ds(0, fs_count - 1)], x_sem.at[2])
    for m, held in enumerate((gate_send, up_send, down_send)):
        wait_bytes(held.at[pl.ds(0, fs_count - 1)], send_sem.at[m])

    def drain(r):
        @pl.when(handles)
        def _():
            wait_bytes(part.at[r, pl.ds(0, fs_count - 1)], rs_send_sem.at[r])
            passed = jnp.logical_and(detours(r), jnp.logical_not(at_bridge))

            @pl.when(passed)
            def _():
                relay_copy(r).wait_send()

            for q in range(pairs):
                tp = base_of(r) // share + q

                @pl.when(jnp.logical_not(jnp.logical_or(passed, is_self(handled, tp))))
                def _(q=q):
                    wait_bytes(total.at[r, q], home_send.at[r, q])

        @pl.when(jnp.logical_not(handles))
        def _():
            wait_bytes(part.at[r], rs_send_sem.at[r])

    loop(rounds, drain)


def per_device(tokens, routes, route_logits, norm_gain, gate_weight, up_weight, down_weight):
    experts, width, columns = gate_weight.shape
    fs_count, tp_count = lax.axis_size("fs"), lax.axis_size("tp")
    spread = fs_count // experts
    block = columns // spread
    own, model = tokens.shape
    group = spread * tp_count
    pairs, share = tp_count // 2, fs_count // tp_count
    pieces = max(1, width // 128)
    rows = width // pieces
    rounds = 2 * pieces
    relayed = max(0, rounds - 2)
    depth = max(1, experts // 2 - 1)
    dma = pltpu.SemaphoreType.DMA
    vmem = pl.BlockSpec(memory_space=pltpu.VMEM)
    anywhere = pl.BlockSpec(memory_space=pl.ANY)
    pinned = [pltpu.VMEM((own, model // tp_count), BF16)]
    pinned += [pltpu.VMEM((fs_count, width, block), BF16)] * 3
    spare = [jax.ShapeDtypeStruct((fs_count, width, block), BF16)] * 2
    outs = pl.pallas_call(
        functools.partial(fused_kernel, fs_count, tp_count, experts, pieces, relayed),
        in_specs=[anywhere] * 7,
        out_specs=[vmem] * 4 + [anywhere] * 2,
        out_shape=pinned + spare,
        scratch_shapes=[
            pltpu.VMEM((own, model), BF16),
            pltpu.VMEM((2, own), jnp.int32),
            pltpu.VMEM((2, own), F32),
            pltpu.VMEM((width // 128, 128), F32),
            pltpu.VMEM((2, width, block), F32),
            pltpu.VMEM((fs_count, width, block), BF16),
            pltpu.VMEM((2, width, block), BF16),
            pltpu.VMEM((8, 128), F32),
            pltpu.VMEM((width, 1), F32),
            pltpu.VMEM((share * own, 1), F32),
            pltpu.VMEM((share, own, width), BF16),
            pltpu.VMEM((fs_count, own, width), BF16),
            pltpu.VMEM((fs_count, fs_count, own, width), BF16),
            pltpu.VMEM((2, fs_count * own, block), F32),
            pltpu.VMEM((fs_count * own, block), BF16),
            pltpu.VMEM((rounds, fs_count, pairs, share * own, rows), BF16),
            pltpu.VMEM((rounds, group - 1, pairs, share * own, rows), BF16),
            pltpu.VMEM((rounds, pairs, share * own, rows), BF16),
            pltpu.VMEM((experts, pieces, share * own, rows), BF16),
            pltpu.VMEM((max(1, relayed), depth, pairs, share * own, rows), BF16),
            pltpu.VMEM((8, 128), F32),
            dma((2,)), dma((2,)), dma((3,)), dma((2, fs_count)), dma((pieces, fs_count)),
            dma((6,)), dma((rounds,)), dma((rounds,)), dma((rounds, tp_count // 2)),
            dma((pieces, experts)), dma((max(1, relayed),)), dma((max(1, relayed),)), dma((2,)),
            dma((4,)),
        ],
        compiler_params=pltpu.CompilerParams(
            collective_id=0, has_side_effects=True, vmem_limit_bytes=VMEM_BYTES - 6 * fs_count * width * block
        ),
    )(
        tokens, routes.T, route_logits.T, norm_gain.reshape(-1, 128),
        gate_weight, up_weight, down_weight,
    )
    mixed, *landings = pl.pallas_call(
        store_kernel,
        in_specs=[vmem] * 4,
        out_specs=[anywhere] * 4,
        out_shape=[jax.ShapeDtypeStruct(x.shape, x.dtype) for x in outs[:4]],
        scratch_shapes=[dma((4,))],
        compiler_params=pltpu.CompilerParams(vmem_limit_bytes=4 * 1024 * 1024),
    )(*outs[:4])
    return (mixed, *(x.reshape(1, fs_count * width, block) for x in landings))


def solution(mesh):
    in_specs = (
        P("fs", None),
        P("fs", None),
        P("fs", None),
        P("fs"),
        P(None, "fs", "tp"),
        P(None, "fs", "tp"),
        P(None, "fs", "tp"),
    )
    out_specs = (P("fs", "tp"), P("tp", None, "fs"), P("tp", None, "fs"), P("tp", None, "fs"))
    return jax.shard_map(
        per_device, mesh=mesh, in_specs=in_specs, out_specs=out_specs, check_vma=False
    )
```

```python
import functools

import jax
import jax.numpy as jnp
from jax import lax
from jax.experimental import pallas as pl
from jax.experimental.pallas import tpu as pltpu
from jax.sharding import PartitionSpec as P

MESH = pl.DeviceIdType.MESH
F32, BF16 = jnp.float32, jnp.bfloat16
VMEM_BYTES = 60 * 1024 * 1024


def wait_bytes(ref, sem):
    pltpu.make_async_copy(ref, ref, sem).wait()


def loop(count, body):
    def step(i, carry):
        body(i)
        return carry

    lax.fori_loop(0, count, step, 0)


def store_kernel(*refs):
    count = (len(refs) - 1) // 2
    held, out, sem = refs[:count], refs[count : 2 * count], refs[-1]
    pltpu.make_async_copy(held[0], out[0], sem.at[0]).start()
    for i in range(1, count):
        for g in range(held[i].shape[0]):
            pltpu.make_async_copy(held[i].at[g], out[i].at[g], sem.at[i]).start()
    for i in range(count):
        pltpu.make_async_copy(held[i], out[i], sem.at[i]).wait()


def fused_kernel(
    fs_count, tp_count, experts, pieces, relayed,
    tok_hbm, routes_hbm, logits_hbm, gain_hbm, gate_hbm, up_hbm, down_hbm,
    mixed_out, gate_out, up_out, down_out, up_send, down_send,
    tok_ref, routes_ref, logits_ref, gain_ref, stage, gate_send, packed, turn, gain_col,
    share_col,
    xown, xcol, x_all, act, hidden, part, rs_recv, total, home, relay, shares,
    load_sem, store_sem, send_sem, recv_sem, down_sem, x_sem,
    rs_send_sem, rs_recv_sem, home_send, home_recv, relay_send, relay_recv, share_sem, small_sem,
):
    me, my_tp = lax.axis_index("fs"), lax.axis_index("tp")
    spread = fs_count // experts
    mine, inner = me // spread, lax.rem(me, spread)
    group = spread * tp_count
    index = inner * tp_count + my_tp
    half = fs_count // 2
    side = me // half
    share = fs_count // tp_count
    own, model = tok_ref.shape
    width, block = stage.shape[1], stage.shape[2]
    rows = width // pieces
    tokens = fs_count * own
    pairs = tp_count // 2
    rounds = 2 * pieces
    planes = experts // 2

    def seat(z):
        return lax.rem(z, planes) * 2 + z // planes

    handled = (lax.rem(my_tp, 2) * planes + my_tp // 2) * spread + inner
    handles = my_tp < experts
    own_home = jnp.logical_and(handles, handled == me)
    depth = experts // 2 - 1
    bridge = jnp.where(side == 0, depth, experts - 1 - depth)
    far_bridge = experts - 1 - bridge
    at_bridge = mine == bridge
    far_home = handled // half != side
    near_slots = pl.ds(0, half - 1)
    far_slots = pl.ds((1 - side) * half, half)

    def ranked(k):
        return jnp.where(side == 0, k, experts - 1 - k)

    def send_order(step):
        return lax.rem(me + half + step, fs_count)

    def near_source(k):
        return side * half + lax.rem(me + 2 * half - 1 - k, half)

    def far_source(k):
        return (1 - side) * half + lax.rem(me + half - k, half)

    def gather_peer(s):
        other = lax.rem(my_tp * share + lax.rem(inner, share) + s, fs_count)
        fs = mine * spread + (inner // share) * share + lax.rem(other, share)
        return fs, other // share

    def plane_peer(i):
        return mine * spread + lax.rem(i, spread), seat(i // spread)

    small = [
        pltpu.make_async_copy(hbm, ref, small_sem.at[i])
        for i, (hbm, ref) in enumerate(
            (
                (gain_hbm, gain_ref), (tok_hbm, tok_ref), (routes_hbm, routes_ref),
                (logits_hbm, logits_ref),
            )
        )
    ]
    barrier = pltpu.get_barrier_semaphore()

    def signal(fs, tp):
        pl.semaphore_signal(
            barrier, inc=1, device_id={"fs": fs, "tp": tp}, device_id_type=MESH
        )

    def load(hbm, step, slot):
        dst = send_order(step)
        column = pl.multiple_of(lax.rem(dst, spread) * block, block)
        return pltpu.make_async_copy(
            hbm.at[dst // spread, :, pl.ds(column, block)], stage.at[slot], load_sem.at[slot]
        )

    small[0].start()
    load(gate_hbm, 0, 0).start()
    for copy in small[1:]:
        copy.start()
    home[...] = jnp.zeros_like(home)
    loop(fs_count - 1, lambda s: signal(lax.rem(me + 1 + s, fs_count), my_tp))

    def greet(s):
        other = lax.rem(index + 1 + s, group)
        signal(mine * spread + other // tp_count, lax.rem(other, tp_count))

    loop(group - 1, greet)

    def sender_of(e):
        return e * spread + inner, seat(mine)

    def is_self(fs, tp):
        return jnp.logical_and(fs == me, tp == my_tp)

    for e in range(experts):
        fs, tp = sender_of(e)

        @pl.when(jnp.logical_not(is_self(fs, tp)))
        def _(fs=fs, tp=tp):
            signal(fs, tp)

    turn[...] = jnp.zeros_like(turn)
    small[0].wait()
    turn[: gain_ref.shape[0]] = gain_ref[...]
    turned = turn[...].T
    for q in range(width // 128):
        gain_col[q * 128 : (q + 1) * 128] = turned[:, q : q + 1]

    load(gate_hbm, 0, 0).wait()
    load(gate_hbm, 1, 1).start()
    gate_send[send_order(0)] = (stage[0] * gain_col[...]).astype(BF16)
    load(gate_hbm, 1, 1).wait()
    load(gate_hbm, 2, 0).start()
    gate_send[send_order(1)] = (stage[1] * gain_col[...]).astype(BF16)
    for copy in small[1:]:
        copy.wait()
    tok = tok_ref[...].astype(F32)
    scale = lax.rsqrt(jnp.mean(tok * tok, axis=1, keepdims=True) + 1e-05)
    for j in range(share):
        column = pl.multiple_of((my_tp * share + j) * width, width)
        cols = tok_ref[:, pl.ds(column, width)].astype(F32)
        xown[j] = (cols * scale).astype(BF16)
    xcol[me] = xown[lax.rem(inner, share)]

    homes = jnp.where(handles, tp_count, 0) - jnp.where(own_home, 1, 0)
    pl.semaphore_wait(barrier, fs_count + group - 2 + homes)

    def block_copy(m, held, out, dst):
        return pltpu.make_async_remote_copy(
            src_ref=held.at[dst], dst_ref=out.at[me], send_sem=send_sem.at[m],
            recv_sem=recv_sem.at[m, me], device_id={"fs": dst}, device_id_type=MESH,
        )

    block_copy(0, gate_send, gate_out, send_order(0)).start()
    block_copy(0, gate_send, gate_out, send_order(1)).start()

    def x_send(dst):
        pltpu.make_async_remote_copy(
            src_ref=xown.at[lax.rem(lax.rem(dst, spread), share)], dst_ref=xcol.at[me],
            send_sem=x_sem.at[0], recv_sem=x_sem.at[1], device_id={"fs": dst},
            device_id_type=MESH,
        ).start()

    loop(spread, lambda h: x_send(far_bridge * spread + lax.rem(inner + h, spread)))
    loop(half - 1, lambda s: x_send(side * half + lax.rem(me + 1 + s, half)))

    def shares_copy(fs):
        return pltpu.make_async_remote_copy(
            src_ref=turn, dst_ref=shares, send_sem=share_sem.at[0], recv_sem=share_sem.at[1],
            device_id={"fs": fs}, device_id_type=MESH,
        )

    def for_planes(action):
        for e in range(experts):
            fs = e * spread + inner

            @pl.when(jnp.logical_and(my_tp == seat(mine), fs != me))
            def _(fs=fs):
                action(fs)

    turn[...] = jnp.zeros_like(turn)
    first, second = logits_ref[0:1], logits_ref[1:2]
    share_first = 1.0 / (1.0 + jnp.exp(second - first))
    share_second = 1.0 / (1.0 + jnp.exp(first - second))
    for e in range(experts):
        turn[e : e + 1, :own] = jnp.where(routes_ref[0:1] == e, share_first, 0.0) + jnp.where(
            routes_ref[1:2] == e, share_second, 0.0
        )
    for_planes(lambda fs: shares_copy(fs).start())

    @pl.when(own_home)
    def _():
        shares[...] = turn[...]

    def piece_copy(p, dst):
        span = pl.ds(pl.multiple_of(p * rows, rows), rows)
        return pltpu.make_async_remote_copy(
            src_ref=down_send.at[dst, span], dst_ref=down_out.at[me, span],
            send_sem=send_sem.at[2], recv_sem=down_sem.at[p, me], device_id={"fs": dst},
            device_id_type=MESH,
        )

    def convert(m, hbm, following):
        begin = 2 if m == 0 else 0

        def body(i):
            step = i + begin
            slot = lax.rem(m * fs_count + step, 2)
            dst = send_order(step)

            @pl.when(step + 1 < fs_count)
            def _():
                load(hbm, step + 1, 1 - slot).start()

            if following is not None:

                @pl.when(step + 1 == fs_count)
                def _():
                    load(following, 0, 1 - slot).start()

            load(hbm, step, slot).wait()
            held, out = ((gate_send, gate_out), (up_send, up_out), (down_send, down_out))[m]
            block_f32 = stage[slot]
            if m < 2:
                block_f32 = block_f32 * gain_col[...]
            rounded = block_f32.astype(BF16)

            @pl.when(dst == me)
            def _():
                out[me] = rounded

            @pl.when(dst != me)
            def _():
                if m == 0:
                    held[dst] = rounded
                    block_copy(m, held, out, dst).start()
                else:
                    packed[slot] = rounded
                    store(held, step).start()

            if m > 0:

                @pl.when(jnp.logical_and(step > 0, send_order(step - 1) != me))
                def _():
                    stored(m, held, out, step - 1)

        def store(held, step):
            slot = lax.rem(m * fs_count + step, 2)
            return pltpu.make_async_copy(
                packed.at[slot], held.at[send_order(step)], store_sem.at[slot]
            )

        def stored(m, held, out, step):
            store(held, step).wait()
            if m == 1:
                block_copy(m, held, out, send_order(step)).start()

        loop(fs_count - begin, body)
        if m > 0:
            held, out = ((up_send, up_out), (down_send, down_out))[m - 1]

            @pl.when(send_order(fs_count - 1) != me)
            def _():
                stored(m, held, out, fs_count - 1)

    convert(0, gate_hbm, up_hbm)

    def x_forward(k):
        return pltpu.make_async_remote_copy(
            src_ref=xcol.at[far_slots], dst_ref=xcol.at[far_slots], send_sem=x_sem.at[4],
            recv_sem=x_sem.at[5], device_id={"fs": ranked(k) * spread + inner},
            device_id_type=MESH,
        )

    @pl.when(at_bridge)
    def _():
        wait_bytes(xcol.at[pl.ds(0, fs_count - 1)], x_sem.at[1])
        loop(depth, lambda k: x_forward(k).start())

    @pl.when(jnp.logical_not(at_bridge))
    def _():
        wait_bytes(xcol.at[near_slots], x_sem.at[1])
        wait_bytes(xcol.at[far_slots], x_sem.at[5])

    held_part = my_tp * share + lax.rem(inner, share)

    def x_gather(s):
        fs, tp = gather_peer(s + 1)
        pltpu.make_async_remote_copy(
            src_ref=xcol, dst_ref=x_all.at[held_part], send_sem=x_sem.at[2],
            recv_sem=x_sem.at[3], device_id={"fs": fs, "tp": tp}, device_id_type=MESH,
        ).start()

    loop(fs_count - 1, x_gather)
    x_all[held_part] = xcol[...]

    convert(1, up_hbm, down_hbm)
    convert(2, down_hbm, None)
    def pc(p, s):
        dst = send_order(s)

        @pl.when(dst != me)
        def _():
            piece_copy(p, dst).start()

    loop(pieces, lambda p: loop(fs_count, lambda s: pc(p, s)))

    wait_bytes(x_all.at[pl.ds(0, fs_count - 1)], x_sem.at[3])

    def project(m, out):
        act[m] = jnp.zeros_like(act[m])

        def body(k):
            g = jnp.where(k < half, near_source(k), far_source(k - half))

            @pl.when(g != me)
            def _():
                wait_bytes(out.at[g], recv_sem.at[m, g])

            x = x_all[g].astype(F32).reshape(tokens, width).astype(BF16)
            act[m] += jnp.dot(x, out[g], preferred_element_type=F32)

        loop(fs_count, body)

    project(0, gate_out)
    project(1, up_out)
    gate = act[0]
    hidden[...] = (gate / (1.0 + jnp.exp(-gate)) * act[1]).astype(BF16)

    def base_of(r):
        return jnp.where(lax.rem(r, 2) == 0, side, 1 - side) * half

    def finish(r):
        wait_bytes(rs_recv.at[r], rs_recv_sem.at[r])

        def add(s, acc):
            return acc + rs_recv[r, s].astype(F32)

        acc = lax.fori_loop(0, group - 1, add, part[r, handled].astype(F32))
        total[r] = (acc * share_col[...][None]).astype(BF16)
        if relayed == 0:
            send_home(r)
            return
        detour = detours(r)

        @pl.when(jnp.logical_and(detour, jnp.logical_not(at_bridge)))
        def _():
            relay_copy(r).start()

        @pl.when(jnp.logical_not(detour))
        def _():
            send_home(r)

    def detours(r):
        return jnp.logical_and(far_home, r < relayed)

    def relay_copy(r):
        return pltpu.make_async_remote_copy(
            src_ref=total.at[r], dst_ref=relay.at[r, jnp.where(side == 0, mine, experts - 1 - mine)],
            send_sem=relay_send.at[r], recv_sem=relay_recv.at[r],
            device_id={"fs": bridge * spread + inner}, device_id_type=MESH,
        )

    def cross(r):
        wait_bytes(relay.at[r], relay_recv.at[r])
        acc = total[r].astype(F32)
        for k in range(depth):
            acc = acc + relay[r, k].astype(F32)
        total[r] = acc.astype(BF16)
        send_home(r)

    def send_home(r):
        p = r // 2
        for q in range(pairs):
            tp = base_of(r) // share + q

            @pl.when(is_self(handled, tp))
            def _(q=q):
                home[mine, p] = total[r, q]

            @pl.when(jnp.logical_not(is_self(handled, tp)))
            def _(q=q, tp=tp):
                home_copy(r, q, tp).start()

    def home_copy(r, q, tp):
        return pltpu.make_async_remote_copy(
            src_ref=total.at[r, q], dst_ref=home.at[mine, r // 2],
            send_sem=home_send.at[r, q], recv_sem=home_recv.at[r // 2, mine],
            device_id={"fs": handled, "tp": tp}, device_id_type=MESH,
        )

    column = lax.rem(me, half)
    first_cut = jnp.where(jnp.logical_or(column < share // 2, column >= half - share // 2), 1, 0)

    def run_round(r):
        p = r // 2
        span = pl.ds(pl.multiple_of(p * rows, rows), rows)

        def project_back(g):
            @pl.when(g != me)
            def _():
                wait_bytes(down_out.at[g, span], down_sem.at[p, g])

            out = lax.dot_general(
                hidden[...], down_out[g, span], (((1,), (1,)), ((), ())),
                preferred_element_type=F32,
            )
            return out.reshape(fs_count, own, rows)

        def cut(k):
            q = lax.rem(k + first_cut, pairs)
            base = base_of(r) + q * share
            outs = [project_back(base + j) for j in range(share)]
            part[r, :, q] = jnp.concatenate(outs, axis=1).astype(BF16)

            def rs_send(s):
                i = lax.rem(me + 1 + s, fs_count)
                fs, tp = plane_peer(i)

                @pl.when(jnp.logical_not(is_self(fs, tp)))
                def _():
                    place = lax.rem(i, spread) * tp_count + tp
                    slot = lax.rem(index + 2 * group - place - 1, group)
                    pltpu.make_async_remote_copy(
                        src_ref=part.at[r, i, q], dst_ref=rs_recv.at[r, slot, q],
                        send_sem=rs_send_sem.at[r], recv_sem=rs_recv_sem.at[r],
                        device_id={"fs": fs, "tp": tp}, device_id_type=MESH,
                    ).start()

            loop(fs_count, rs_send)

        if relayed > 0:
            crossing = jnp.logical_and(jnp.logical_and(handles, far_home), at_bridge)

            @pl.when(jnp.logical_and(crossing, r == rounds - 2))
            def _():
                loop(relayed - 2, cross)

            @pl.when(jnp.logical_and(crossing, r == rounds - 1))
            def _():
                loop(2, lambda k: cross(relayed - 2 + k))

        loop(pairs, cut)

        @pl.when(jnp.logical_and(r > 0, handles))
        def _():
            finish(r - 1)

    @pl.when(jnp.logical_and(handles, handled != me))
    def _():
        wait_bytes(shares, share_sem.at[1])

    @pl.when(handles)
    def _():
        columns = shares[...].T
        lanes = lax.broadcasted_iota(jnp.int32, columns.shape, 1)
        scale = jnp.sum(jnp.where(lanes == mine, columns, 0.0), axis=1, keepdims=True)
        for j in range(share):
            share_col[j * own : (j + 1) * own] = scale[:own]

    loop(rounds, run_round)

    @pl.when(handles)
    def _():
        finish(rounds - 1)

    for p in range(pieces):
        mixed = [jnp.zeros((own, rows), F32)] * share
        for e in range(experts):

            sent = jnp.logical_not(is_self(*sender_of(e)))
            if relayed > 0:
                apart = jnp.where(my_tp // pairs == e // (depth + 1), 0, 1)
                skipped = jnp.logical_and(side != e // (depth + 1), 2 * p + apart < relayed)
                sent = jnp.logical_and(
                    sent, jnp.logical_or(jnp.logical_not(skipped), e == far_bridge)
                )

            @pl.when(sent)
            def _(e=e, p=p):
                wait_bytes(home.at[e, p], home_recv.at[p, e])

            landed = home[e, p].astype(F32)
            for j in range(share):
                mixed[j] = mixed[j] + landed[j * own : (j + 1) * own]
        for j in range(share):
            column = j * width + p * rows
            mixed_out[:, column : column + rows] = mixed[j].astype(BF16)

    wait_bytes(xcol.at[pl.ds(0, spread + half - 1)], x_sem.at[0])
    for_planes(lambda fs: shares_copy(fs).wait_send())

    @pl.when(at_bridge)
    def _():
        loop(depth, lambda k: x_forward(k).wait_send())

    wait_bytes(x_all.at[pl.ds(0, fs_count - 1)], x_sem.at[2])
    for m, held in enumerate((gate_send, up_send, down_send)):
        wait_bytes(held.at[pl.ds(0, fs_count - 1)], send_sem.at[m])

    def drain(r):
        @pl.when(handles)
        def _():
            wait_bytes(part.at[r, pl.ds(0, fs_count - 1)], rs_send_sem.at[r])
            passed = jnp.logical_and(detours(r), jnp.logical_not(at_bridge))

            @pl.when(passed)
            def _():
                relay_copy(r).wait_send()

            for q in range(pairs):
                tp = base_of(r) // share + q

                @pl.when(jnp.logical_not(jnp.logical_or(passed, is_self(handled, tp))))
                def _(q=q):
                    wait_bytes(total.at[r, q], home_send.at[r, q])

        @pl.when(jnp.logical_not(handles))
        def _():
            wait_bytes(part.at[r], rs_send_sem.at[r])

    loop(rounds, drain)


def per_device(tokens, routes, route_logits, norm_gain, gate_weight, up_weight, down_weight):
    experts, width, columns = gate_weight.shape
    fs_count, tp_count = lax.axis_size("fs"), lax.axis_size("tp")
    spread = fs_count // experts
    block = columns // spread
    own, model = tokens.shape
    group = spread * tp_count
    pairs, share = tp_count // 2, fs_count // tp_count
    pieces = max(1, width // 128)
    rows = width // pieces
    rounds = 2 * pieces
    relayed = max(0, rounds - 2)
    depth = max(1, experts // 2 - 1)
    dma = pltpu.SemaphoreType.DMA
    vmem = pl.BlockSpec(memory_space=pltpu.VMEM)
    anywhere = pl.BlockSpec(memory_space=pl.ANY)
    pinned = [pltpu.VMEM((own, model // tp_count), BF16)]
    pinned += [pltpu.VMEM((fs_count, width, block), BF16)] * 3
    spare = [jax.ShapeDtypeStruct((fs_count, width, block), BF16)] * 2
    outs = pl.pallas_call(
        functools.partial(fused_kernel, fs_count, tp_count, experts, pieces, relayed),
        in_specs=[anywhere] * 7,
        out_specs=[vmem] * 4 + [anywhere] * 2,
        out_shape=pinned + spare,
        scratch_shapes=[
            pltpu.VMEM((own, model), BF16),
            pltpu.VMEM((2, own), jnp.int32),
            pltpu.VMEM((2, own), F32),
            pltpu.VMEM((width // 128, 128), F32),
            pltpu.VMEM((2, width, block), F32),
            pltpu.VMEM((fs_count, width, block), BF16),
            pltpu.VMEM((2, width, block), BF16),
            pltpu.VMEM((8, 128), F32),
            pltpu.VMEM((width, 1), F32),
            pltpu.VMEM((share * own, 1), F32),
            pltpu.VMEM((share, own, width), BF16),
            pltpu.VMEM((fs_count, own, width), BF16),
            pltpu.VMEM((fs_count, fs_count, own, width), BF16),
            pltpu.VMEM((2, fs_count * own, block), F32),
            pltpu.VMEM((fs_count * own, block), BF16),
            pltpu.VMEM((rounds, fs_count, pairs, share * own, rows), BF16),
            pltpu.VMEM((rounds, group - 1, pairs, share * own, rows), BF16),
            pltpu.VMEM((rounds, pairs, share * own, rows), BF16),
            pltpu.VMEM((experts, pieces, share * own, rows), BF16),
            pltpu.VMEM((max(1, relayed), depth, pairs, share * own, rows), BF16),
            pltpu.VMEM((8, 128), F32),
            dma((2,)), dma((2,)), dma((3,)), dma((2, fs_count)), dma((pieces, fs_count)),
            dma((6,)), dma((rounds,)), dma((rounds,)), dma((rounds, tp_count // 2)),
            dma((pieces, experts)), dma((max(1, relayed),)), dma((max(1, relayed),)), dma((2,)),
            dma((4,)),
        ],
        compiler_params=pltpu.CompilerParams(
            collective_id=0, has_side_effects=True, vmem_limit_bytes=VMEM_BYTES - 6 * fs_count * width * block
        ),
    )(
        tokens, routes.T, route_logits.T, norm_gain.reshape(-1, 128),
        gate_weight, up_weight, down_weight,
    )
    mixed, *landings = pl.pallas_call(
        store_kernel,
        in_specs=[vmem] * 4,
        out_specs=[anywhere] * 4,
        out_shape=[jax.ShapeDtypeStruct(x.shape, x.dtype) for x in outs[:4]],
        scratch_shapes=[dma((4,))],
        compiler_params=pltpu.CompilerParams(vmem_limit_bytes=4 * 1024 * 1024),
    )(*outs[:4])
    return (mixed, *(x.reshape(1, fs_count * width, block) for x in landings))


def solution(mesh):
    in_specs = (
        P("fs", None),
        P("fs", None),
        P("fs", None),
        P("fs"),
        P(None, "fs", "tp"),
        P(None, "fs", "tp"),
        P(None, "fs", "tp"),
    )
    out_specs = (P("fs", "tp"), P("tp", None, "fs"), P("tp", None, "fs"), P("tp", None, "fs"))
    return jax.shard_map(
        per_device, mesh=mesh, in_specs=in_specs, out_specs=out_specs, check_vma=False
    )
```
